32 devices in a mesh: sp: 8 (over z, y), tp: 4 (over x, core).
Axes of the slice: x: 2, y: 2, z: 4, core: 2. Of those that a mesh axis runs over, the one named last changes fastest.
Arguments:
- tokens: bfloat16 [4096, 2048], P('sp'), may hold values from -24 to 24
- w_query: bfloat16 [2048, 1536], P('sp', 'tp'), as said below
- w_key: bfloat16 [2048, 1536], P('sp', 'tp'), as said below
- w_value: bfloat16 [2048, 1536], P('sp', 'tp'), may hold values from -0.125 to 0.125
- w_out: bfloat16 [512, 2048], P('tp', 'sp'), may hold values from -1.5 to 1.5
Outputs:
- mixed: bfloat16 [4096, 2048], P(('sp', 'tp'))
The draws below stay inside these ranges and needn't reach their ends.
Inputs may be any that keep to these rules, and one draw needn't show every extreme that they name: `w_query`: every entry lies within 4 / sqrt(2048) of zero. `w_key`: every entry lies within 4 / sqrt(2048) of zero.
All inputs are finite; a program needn't handle non-finite values.
Results may differ from the reference program's by a relative error of at most 0.025.
Values may be sent and summed in bfloat16 or wider, within the bound.
A program may use at most 64 MiB of HBM per device.

```python
import math
import jax
import jax.numpy as jnp
from jax import lax

D = 2048
HEADS = 4
GROUPS = 3
DH = 128
WIN1 = 128
WIN2 = 512
WIN3 = 2048
SECOND_DILATION = 4
THIRD_DILATION = 16
SEQ = 4096


def shared_query(key):
    return jax.random.normal(jax.random.fold_in(key, 101), (D, HEADS * GROUPS * DH), jnp.float32)


def draw_tokens(key, part):
    drawn = jax.random.normal(jax.random.fold_in(key, 1), (SEQ, D), jnp.float32)
    return jnp.clip(drawn, -24.0, 24.0).astype(jnp.bfloat16)


def draw_w_query(key, part):
    limit = 4.0 * D ** (-0.5)
    return jnp.clip(shared_query(key) * D ** (-0.5), -limit, limit).astype(jnp.bfloat16)


def draw_w_key(key, part):
    limit = 4.0 * D ** (-0.5)
    own_part = jax.random.normal(jax.random.fold_in(key, 202), (D, HEADS * GROUPS * DH), jnp.float32)
    return jnp.clip(own_part * D ** (-0.5), -limit, limit).astype(jnp.bfloat16)


def shard_levels(own_key, shape, cuts, smallest, top_value):
    level, own = 1.0, jax.random.fold_in(own_key, 6)
    for axis_at, blocks in cuts:
        steps = jnp.exp(jax.random.uniform(jax.random.fold_in(own, axis_at), (blocks,), jnp.float32, smallest / len(cuts), top_value / len(cuts)))
        level = level * jnp.repeat(steps, shape[axis_at] // blocks).reshape([-1 if axis == axis_at else 1 for axis in range(len(shape))])
    return level


def scatter_about(own_key, dims, scale, bound, cuts=(), kind=jnp.bfloat16):
    loudness = shard_levels(own_key, dims, cuts, -0.22, 0.18) if cuts else 1.0
    drawn = jax.random.normal(own_key, dims, jnp.float32) * scale * loudness
    return jnp.minimum(jnp.maximum(drawn, -bound), bound).astype(kind)


def setup_inputs(seed: int = 0) -> dict:
    arg_keys = jax.random.split(jax.random.key(seed), 6)
    tokens = draw_tokens(jax.random.fold_in(arg_keys[5], 71), 0)
    w_query = draw_w_query(jax.random.fold_in(arg_keys[5], 71), 0)
    w_key = draw_w_key(jax.random.fold_in(arg_keys[5], 71), 0)
    w_value = scatter_about(arg_keys[3], (D, HEADS * GROUPS * DH), D ** -0.5, 0.125, ((0, 8), (1, 4)))
    w_out = scatter_about(arg_keys[4], (HEADS * DH, D), 0.35, 1.5, ((0, 4), (1, 8)))
    return dict(tokens=tokens, w_query=w_query, w_key=w_key, w_value=w_value, w_out=w_out)


ROPE_BASE = 500000.0


def rotate(projected):
    seq_len = projected.shape[0]
    head_size = projected.shape[-1]
    half_size = head_size // 2
    positions = jnp.arange(seq_len, dtype=jnp.int32).astype(jnp.float32)
    frequency = 1.0 / (ROPE_BASE ** (jnp.arange(0, head_size, 2, dtype=jnp.float32) / head_size))
    angles = (positions[:, None] * frequency[None, :]).reshape(seq_len, 1, 1, half_size)
    cosine = jnp.cos(angles)
    sine_part = jnp.sin(angles)
    first_half = projected[..., :half_size]
    second_half = projected[..., half_size:]
    return jnp.concatenate([first_half * cosine - second_half * sine_part,
                            second_half * cosine + first_half * sine_part], axis=-1)


def window_attend(queries, keys, values, window, stride):
    seq_len, heads, head_size = queries.shape
    block_rows = math.gcd(seq_len, 512)
    block_list = seq_len // block_rows
    key_pad = jnp.pad(keys, ((window, 0), (0, 0), (0, 0)))
    value_pad = jnp.pad(values, ((window, 0), (0, 0), (0, 0)))
    query_blocks = queries.reshape(block_list, block_rows, heads, head_size)

    def one_block(operands):
        query_block, block_index = operands
        begin = (block_index * block_rows).astype(jnp.int32)
        key_slab = lax.dynamic_slice_in_dim(key_pad, begin, block_rows + window, 0)
        value_band = lax.dynamic_slice_in_dim(value_pad, begin, block_rows + window, 0)
        scores = jnp.einsum('qhe,khe->hqk', query_block.astype(jnp.float32),
                            key_slab.astype(jnp.float32)) * (head_size ** -0.5)
        query_pos = begin + jnp.arange(block_rows, dtype=jnp.int32)
        key_pos = begin - window + jnp.arange(block_rows + window, dtype=jnp.int32)
        spacing = query_pos[:, None] - key_pos[None, :]
        allowed = (spacing >= 0) & (spacing <= window) & (spacing % stride == 0) & (key_pos[None, :] >= 0)
        scores = jnp.where(allowed[None], scores, -jnp.inf)
        row_max = jnp.max(scores, axis=-1)
        exponent = jnp.exp(scores - row_max[..., None])
        totals = jnp.sum(exponent, axis=-1)
        probs = lax.optimization_barrier((exponent / totals[..., None]).astype(jnp.bfloat16))
        mixed = jnp.einsum('hqk,khe->qhe', probs.astype(jnp.float32), value_band.astype(jnp.float32))
        return mixed, jnp.transpose(row_max + jnp.log(totals))

    mixed, log_totals = lax.map(one_block, (query_blocks, jnp.arange(block_list, dtype=jnp.int32)))
    return mixed.reshape(seq_len, heads, head_size), log_totals.reshape(seq_len, heads)


def reference(tokens, w_query, w_key, w_value, w_out):
    seq_len = tokens.shape[0]
    head_shape = (seq_len, HEADS, GROUPS, DH)
    query_raw = jnp.dot(tokens, w_query, preferred_element_type=jnp.float32).reshape(head_shape)
    key_raw = jnp.dot(tokens, w_key, preferred_element_type=jnp.float32).reshape(head_shape)
    values = lax.optimization_barrier(
        jnp.dot(tokens, w_value, preferred_element_type=jnp.float32).astype(jnp.bfloat16)).reshape(head_shape)
    queries = lax.optimization_barrier(rotate(query_raw).astype(jnp.bfloat16))
    keys = lax.optimization_barrier(rotate(key_raw).astype(jnp.bfloat16))
    windows = (WIN1, WIN2, WIN3)
    step_sizes = (1, SECOND_DILATION, THIRD_DILATION)
    outputs = []
    log_totals = []
    for group_index in range(GROUPS):
        group_out, log_total = window_attend(queries[:, :, group_index], keys[:, :, group_index],
                                             values[:, :, group_index], windows[group_index],
                                             step_sizes[group_index])
        outputs.append(group_out)
        log_totals.append(log_total)
    group_weights = jax.nn.softmax(jnp.stack(log_totals), axis=0)
    merged = jnp.sum(group_weights[..., None] * jnp.stack(outputs), axis=0).astype(jnp.bfloat16)
    merged = merged.reshape(seq_len, HEADS * DH)
    return jnp.dot(merged, w_out, preferred_element_type=jnp.float32).astype(jnp.bfloat16)
```

```python
import functools
import math

import jax
import jax.numpy as jnp
from jax import lax
from jax.experimental import pallas as pl
from jax.experimental.pallas import tpu as pltpu
from jax.sharding import PartitionSpec as P

GROUPS = 3
DH = 128
WIN1 = 128
WIN2 = 512
WIN3 = 2048
SECOND_DILATION = 4
THIRD_DILATION = 16


ROPE_BASE = 500000.0


def from_behind(block, axis, distance):
    devices = range(lax.axis_size(axis))
    route = [(i - distance, i) for i in devices if i - distance in devices]
    return lax.ppermute(block, axis, route)


def rotate(projected, offset):
    tok_rows = projected.shape[0]
    head_size = projected.shape[-1]
    half_size = head_size // 2
    positions = (offset + jnp.arange(tok_rows, dtype=jnp.int32)).astype(jnp.float32)
    frequency = 1.0 / ROPE_BASE ** (jnp.arange(0, head_size, 2, dtype=jnp.float32) / head_size)
    angles = (positions[:, None] * frequency[None, :]).reshape(tok_rows, 1, 1, half_size)
    cosine = jnp.cos(angles)
    sine_part = jnp.sin(angles)
    first_half = projected[..., :half_size]
    second_half = projected[..., half_size:]
    return jnp.concatenate(
        [
            first_half * cosine - second_half * sine_part,
            second_half * cosine + first_half * sine_part,
        ],
        axis=-1,
    )


def window_attend(query_part, buffer, steps, stride, offset):
    tok_rows, heads_here, head_size = query_part.shape
    sub_rows = tok_rows // stride
    key_rows = buffer.shape[1] // stride
    query_sub = query_part.reshape(sub_rows, stride, heads_here, head_size).transpose(1, 2, 0, 3)
    pair_sub = buffer.reshape(2, key_rows, stride, heads_here, head_size).transpose(0, 2, 3, 1, 4)
    block_rows = math.gcd(sub_rows, steps) if sub_rows > steps else sub_rows
    block_list = sub_rows // block_rows
    query_blocks = query_sub.reshape(stride, heads_here, block_list, block_rows, head_size)
    key_blocks = jnp.stack(
        [
            pair_sub[:, :, :, index * block_rows : index * block_rows + block_rows + steps]
            for index in range(block_list)
        ],
        axis=3,
    )
    scores = jnp.einsum(
        "zhnqe,zhnke->zhnqk", query_blocks, key_blocks[0], preferred_element_type=jnp.float32
    ) * head_size ** (-0.5)
    query_index = (jnp.arange(block_list, dtype=jnp.int32) * block_rows)[
        :, None, None
    ] + jnp.arange(block_rows, dtype=jnp.int32)[None, :, None]
    key_index = (jnp.arange(block_list, dtype=jnp.int32) * block_rows)[:, None, None] + jnp.arange(
        block_rows + steps, dtype=jnp.int32
    )[None, None, :]
    spacing = query_index + steps - key_index
    residue = jnp.arange(stride, dtype=jnp.int32)[:, None, None, None]
    key_position = offset + (key_index[None] - steps) * stride + residue
    allowed = (spacing[None] >= 0) & (spacing[None] <= steps) & (key_position >= 0)
    scores = jnp.where(allowed[:, None], scores, -jnp.inf)
    row_max = jnp.max(scores, axis=-1)
    exponent = jnp.exp(scores - row_max[..., None])
    totals = jnp.sum(exponent, axis=-1)
    probs = (exponent / totals[..., None]).astype(jnp.bfloat16)
    mixed = jnp.einsum(
        "zhnqk,zhnke->zhnqe", probs, key_blocks[1], preferred_element_type=jnp.float32
    )
    mixed = mixed.reshape(stride, heads_here, sub_rows, head_size).transpose(2, 0, 1, 3)
    log_total = (row_max + jnp.log(totals)).reshape(stride, heads_here, sub_rows).transpose(2, 0, 1)
    return (mixed.reshape(tok_rows, heads_here, head_size), log_total.reshape(tok_rows, heads_here))


def reach_back(key_value, distance_max):
    tok_rows = key_value.shape[1]
    gathered = key_value
    pieces_held = 1
    while pieces_held < distance_max + 1:
        slice_share = min(pieces_held, distance_max + 1 - pieces_held)
        arrived = from_behind(
            gathered[:, gathered.shape[1] - slice_share * tok_rows :], "sp", pieces_held
        )
        gathered = jnp.concatenate([arrived, gathered], axis=1)
        pieces_held = pieces_held + slice_share
    return gathered


def on_device(tokens, w_query, w_key, w_value, w_out):
    tok_rows = tokens.shape[0]
    heads_here = w_out.shape[0] // DH
    offset = lax.axis_index("sp") * tok_rows
    weight_parts = (
        lax.all_gather(w_query, "sp", axis=0, tiled=True),
        lax.all_gather(w_key, "sp", axis=0, tiled=True),
        lax.all_gather(w_value, "sp", axis=0, tiled=True),
    )
    query_raw, key_raw, value_raw = tuple(
        (
            jnp.dot(tokens, weight_rows, preferred_element_type=jnp.float32)
            for weight_rows in weight_parts
        )
    )
    head_shape = (tok_rows, heads_here, GROUPS, DH)
    queries = rotate(query_raw.reshape(head_shape), offset).astype(jnp.bfloat16)
    keys_all = rotate(key_raw.reshape(head_shape), offset).astype(jnp.bfloat16)
    values_all = value_raw.astype(jnp.bfloat16).reshape(head_shape)
    windows = (WIN1, WIN2, WIN3)
    step_sizes = (1, SECOND_DILATION, THIRD_DILATION)
    outputs = []
    log_totals = []
    for group_index in range(GROUPS):
        key_value = jnp.stack([keys_all[:, :, group_index], values_all[:, :, group_index]])
        key_value = key_value.reshape(2, tok_rows, heads_here * DH)
        window = windows[group_index]
        if group_index == 0:
            near_rows = from_behind(key_value[:, tok_rows - window :], "sp", 1)
            buffer = jnp.concatenate([near_rows, key_value], axis=1)
        else:
            distance_max = (window + tok_rows - 1) // tok_rows
            buffer = reach_back(key_value, distance_max)
        group_out, log_total = window_attend(
            queries[:, :, group_index],
            buffer,
            window // step_sizes[group_index],
            step_sizes[group_index],
            offset,
        )
        outputs.append(group_out)
        log_totals.append(log_total)
    group_weights = jax.nn.softmax(jnp.stack(log_totals), axis=0)
    merged = jnp.sum(group_weights[..., None] * jnp.stack(outputs), axis=0).astype(jnp.bfloat16)
    merged = merged.reshape(tok_rows, heads_here * DH)
    w_whole = lax.all_gather(w_out, "sp", axis=1, tiled=True)
    return lax.psum_scatter(
        jnp.dot(merged, w_whole, preferred_element_type=jnp.float32).astype(jnp.bfloat16),
        "tp",
        scatter_dimension=0,
        tiled=True,
    )


def layer_kernel(
    nz,
    tokens, w_key, w_value, w_query, w_out, freq, out,
    weights, tok_in, tok_turned, cosine, sine, queries, pair0, send1, near1, far2,
    out_rows, mine, heads_in,
    swap_s, tok_r, w_r, up_s, down_s, side_s, o_r, o_s, o_r2, far_s, far_r, near_s, near_r, head_s, head_r,
):
    tok_rows, depth = tokens.shape
    k_rows, cols = w_key.shape
    sub = tok_rows // THIRD_DILATION
    block = tok_rows // SECOND_DILATION
    tail = WIN1
    sp, tp = lax.axis_index("sp"), lax.axis_index("tp")
    z, y = sp // 2, sp % 2
    x, c = tp // 2, tp % 2
    rank = 2 * z + c
    side = (sp, 2 * x + 1 - c)
    above = (sp + 2, tp)
    below = (sp - 2, tp)
    partner = (2 * z + 1 - y, 2 * x + 1 - c)
    stays = c == y
    has_up, has_down = z < nz - 1, z > 0

    def send(src, dst, s_sem, r_sem, where):
        return pltpu.make_async_remote_copy(
            src_ref=src, dst_ref=dst, send_sem=s_sem, recv_sem=r_sem,
            device_id=where, device_id_type=pl.DeviceIdType.MESH,
        )

    barrier = pltpu.get_barrier_semaphore()

    def greet(where):
        pl.semaphore_signal(barrier, inc=1, device_id=where, device_id_type=pl.DeviceIdType.MESH)

    for dy in range(2):
        for dx in range(2):
            for dc in range(2):
                if dy + dx + dc:
                    greet((2 * z + (y + dy) % 2, 2 * ((x + dx) % 2) + (c + dc) % 2))
    pl.when(has_up)(lambda: greet(above))
    pl.when(has_down)(lambda: greet(below))
    pl.when(has_up & (c == 1))(lambda: greet((sp + 2, 2 * x)))
    pl.when(has_down & (c == 0))(lambda: greet((sp - 2, 2 * x + 1)))
    greeters = 7 + jnp.where(has_up, 1 + c, 0) + jnp.where(has_down, 2 - c, 0)
    pl.semaphore_wait(barrier, greeters)

    parts = (w_key, w_value, w_query)

    def chunk(a, s):
        return weights.at[a, pl.ds(pl.multiple_of(s * k_rows, k_rows), k_rows), :]

    def o_chunk(zz):
        return out_rows.at[c, x, y, zz]

    def swapped(a):
        there = 2 * z + 1 - c
        return send(parts[a], chunk(a, there), swap_s.at[a], w_r.at[a, there], partner)

    def tok_swapped():
        return send(tokens, tok_in, swap_s.at[3], tok_r, partner)

    def kept(a):
        return pltpu.make_async_copy(parts[a], chunk(a, rank), w_r.at[a, rank])

    def o_kept():
        return pltpu.make_async_copy(w_out, o_chunk(z), o_r.at[z])

    @pl.when(stays)
    def _():
        for a in range(3):
            kept(a).start()

    @pl.when(jnp.logical_not(stays))
    def _():
        for a in range(3):
            swapped(a).start()
        tok_swapped().start()

    o_kept().start()

    def go(a, zz, kind):
        s = 2 * zz + c
        ref = chunk(a, s) if a < 3 else o_chunk(zz)
        r_sem = w_r.at[a, s] if a < 3 else o_r.at[zz]
        s_sem = {"up": up_s, "down": down_s, "side": side_s}[kind].at[a, zz]
        return send(ref, ref, s_sem, r_sem, {"up": above, "down": below, "side": side}[kind])

    def own(a):
        if a < 3:
            pl.when(stays)(lambda: kept(a).wait())
            pl.when(jnp.logical_not(stays))(lambda: go(a, z, "side").wait_recv())
        else:
            o_kept().wait()
        pl.when(has_up)(lambda: go(a, z, "up").start())
        pl.when(has_down)(lambda: go(a, z, "down").start())
        if a < 3:
            go(a, z, "side").start()

    def relay(a, d):
        @pl.when(z - d >= 0)
        def _():
            go(a, z - d, "up").wait_recv()
            pl.when(has_up)(lambda: go(a, z - d, "up").start())
            if a < 3:
                go(a, z - d, "side").start()

        @pl.when(z + d < nz)
        def _():
            go(a, z + d, "down").wait_recv()
            pl.when(has_down)(lambda: go(a, z + d, "down").start())
            if a < 3:
                go(a, z + d, "side").start()

    def others(a):
        for zz in range(nz):
            s = 2 * zz + 1 - c
            send(chunk(a, s), chunk(a, s), side_s.at[a, zz], w_r.at[a, s], side).wait_recv()

    def row_time(p):
        b, i = p // sub, p % sub
        return THIRD_DILATION * i + b // 4 + SECOND_DILATION * (b % 4)

    def tail_time(u):
        per = tail // THIRD_DILATION
        b, i = u // per, u % per
        return THIRD_DILATION * (sub - per + i) + b // 4 + SECOND_DILATION * (b % 4) - tok_rows

    own(0)
    own(1)

    def angles(index, carry):
        rows = pl.ds(pl.multiple_of(index * block, block), block)
        p = lax.broadcasted_iota(jnp.int32, (block, DH), 0) + index * block
        angle = (row_time(p) + rank * tok_rows).astype(jnp.float32) * freq[...]
        lane = lax.broadcasted_iota(jnp.int32, (block, DH), 1)
        cosine[rows, :] = jnp.cos(angle)
        turned = jnp.sin(angle)
        sine[rows, :] = jnp.where(lane < DH // 2, -turned, turned)
        return carry

    lax.fori_loop(0, SECOND_DILATION, angles, 0)

    for a in range(2):
        for d in range(1, nz):
            if d == nz - 1 and a == 1:
                own(2)
            relay(a, d)
    relay(2, 1)

    def order(source):
        p = row_time(lax.broadcasted_iota(jnp.int32, (tok_rows, tok_rows), 0))
        t = lax.broadcasted_iota(jnp.int32, (tok_rows, tok_rows), 1)
        pick = jnp.where(p == t, 1.0, 0.0).astype(jnp.bfloat16)

        def piece(index, carry):
            at = pl.ds(pl.multiple_of(index * 256, 256), 256)
            tok_turned[:, at] = jnp.dot(
                pick, source[:, at], preferred_element_type=jnp.float32
            ).astype(jnp.bfloat16)
            return carry

        lax.fori_loop(0, depth // 256, piece, 0)

    pl.when(stays)(lambda: order(tokens))

    @pl.when(jnp.logical_not(stays))
    def _():
        tok_swapped().wait_recv()
        order(tok_in)

    def project(a, store):
        def piece(index, carry):
            rows = pl.ds(pl.multiple_of(index * block, block), block)
            raw = jnp.dot(tok_turned[rows, :], weights[a], preferred_element_type=jnp.float32)
            for g in range(GROUPS):
                part = raw[:, g * DH : (g + 1) * DH]
                if a != 1:
                    part = part * cosine[rows, :] + pltpu.roll(part, DH // 2, 1) * sine[rows, :]
                store(index, rows, g, part)
            return carry

        lax.fori_loop(0, SECOND_DILATION, piece, 0)

    def keep_pair(which):
        def store(index, rows, g, part):
            if g == 2:
                far2[0, which, rows, :] = part.astype(jnp.bfloat16)
            elif g == 1:
                send1[which, rows, :] = part.astype(jnp.bfloat16)
            else:
                pair0[which, rows, :] = part.astype(jnp.bfloat16)
                per = tail // THIRD_DILATION
                last = jnp.concatenate(
                    [part[b * sub + sub - per : (b + 1) * sub] for b in range(4)], axis=0
                )
                at = pl.ds(pl.multiple_of(tok_rows + index * 4 * per, 4 * per), 4 * per)
                send1[which, at, :] = last.astype(jnp.bfloat16)

        return store

    others(0)
    project(0, keep_pair(0))
    others(1)
    project(1, keep_pair(1))

    def far(index, src, dst, where):
        return send(far2.at[src], far2.at[dst], far_s.at[index], far_r.at[dst], where)

    def near(where):
        return send(send1, near1, near_s, near_r, where)

    up_other = (sp + 2, 2 * x)
    pl.when(has_up)(lambda: far(0, 0, 2, above).start())
    pl.when(c == 0)(lambda: far(1, 0, 1, side).start())
    pl.when(c == 0)(lambda: near(side).start())
    pl.when(has_up & (c == 1))(lambda: near(up_other).start())

    for d in range(1, 5):
        @pl.when(rank < d)
        def _(d=d):
            far2[d] = jnp.zeros(far2.shape[1:], far2.dtype)

    @pl.when(rank < 1)
    def _():
        near1[...] = jnp.zeros(near1.shape, near1.dtype)

    for d in range(2, nz):
        relay(2, d)
    own(3)
    for d in range(1, nz):
        relay(3, d)

    @pl.when(has_down)
    def _():
        far(0, 0, 2, above).wait_recv()
        pl.when(has_up)(lambda: far(2, 2, 4, above).start())
        pl.when(c == 0)(lambda: far(3, 2, 3, side).start())
        pl.when(c == 1)(lambda: far(3, 2, 1, side).start())

    def o_y():
        return send(out_rows.at[c, x, y], out_rows.at[c, x, y], o_s.at[0], o_r2.at[0], (2 * z + 1 - y, tp))

    def o_x():
        return send(out_rows.at[c, x], out_rows.at[c, x], o_s.at[1], o_r2.at[1], (sp, 2 * (1 - x) + c))

    def o_c():
        return send(out_rows.at[c], out_rows.at[c], o_s.at[2], o_r2.at[2], side)

    o_y().start()
    others(2)

    def keep_query(index, rows, g, part):
        queries[g, rows, :] = part.astype(jnp.bfloat16)

    project(2, keep_query)
    o_y().wait()
    o_x().start()

    @pl.when(z >= 2)
    def _():
        far(2, 2, 4, above).wait_recv()
        pl.when(c == 1)(lambda: far(4, 4, 3, side).start())

    pl.when(rank >= 1)(lambda: near(side).wait_recv())
    pl.when(rank >= 1)(lambda: far(1, 0, 1, side).wait_recv())
    pl.when(rank >= 3)(lambda: far(4, 4, 3, side).wait_recv())

    scale = DH ** (-0.5)

    def dots(q, k):
        return lax.dot_general(q, k, (((1,), (1,)), ((), ())), preferred_element_type=jnp.float32)

    def soft(scores, allowed, value):
        scores = jnp.where(allowed, scores * scale, -jnp.inf)
        top = jnp.max(scores, axis=-1, keepdims=True)
        weight = jnp.exp(scores - top)
        return top, jnp.sum(weight, axis=-1, keepdims=True), weight.astype(jnp.bfloat16), value

    def iota(shape, axis):
        return lax.broadcasted_iota(jnp.int32, shape, axis)

    def attend(index, carry):
        begin = index * block
        rows = pl.ds(pl.multiple_of(begin, block), block)
        q = queries[0, rows, :]
        tails = pl.ds(tok_rows, tail)
        scores = jnp.concatenate([dots(q, near1[0, tails, :]), dots(q, pair0[0])], axis=1)
        when_q = row_time(iota((block, tail + tok_rows), 0) + begin)
        lane = iota((block, tail + tok_rows), 1)
        when_k = jnp.where(lane < tail, tail_time(lane), row_time(lane - tail))
        gap = when_q - when_k
        ok = (gap >= 0) & (gap <= WIN1) & (when_k + rank * tok_rows >= 0)
        scores = jnp.where(ok, scores * scale, -jnp.inf)
        top0 = jnp.max(scores, axis=-1, keepdims=True)
        weight = jnp.exp(scores - top0)
        sum0 = jnp.sum(weight, axis=-1, keepdims=True)
        weight = weight.astype(jnp.bfloat16)
        got0 = jnp.dot(weight[:, :tail], near1[1, tails, :], preferred_element_type=jnp.float32)
        got0 += jnp.dot(weight[:, tail:], pair0[1], preferred_element_type=jnp.float32)
        q = queries[1, rows, :]
        scores = jnp.concatenate([dots(q, near1[0, rows, :]), dots(q, send1[0, rows, :])], axis=1)
        place = iota((block, 2 * block), 0)
        lane = iota((block, 2 * block), 1)
        step_q = 4 * (place % sub) + place // sub
        inner = lane % block
        step_k = 4 * (inner % sub) + inner // sub + jnp.where(lane < block, -block, 0)
        gap = step_q - step_k
        ok = (gap >= 0) & (gap <= WIN2 // SECOND_DILATION) & (step_k + rank * block >= 0)
        scores = jnp.where(ok, scores * scale, -jnp.inf)
        top1 = jnp.max(scores, axis=-1, keepdims=True)
        weight = jnp.exp(scores - top1)
        sum1 = jnp.sum(weight, axis=-1, keepdims=True)
        weight = weight.astype(jnp.bfloat16)
        got1 = jnp.dot(weight[:, :block], near1[1, rows, :], preferred_element_type=jnp.float32)
        got1 += jnp.dot(weight[:, block:], send1[1, rows, :], preferred_element_type=jnp.float32)
        all_scores = []
        for b in range(4):
            here = pl.ds(pl.multiple_of(begin + b * sub, sub), sub)
            keys = jnp.concatenate([far2[d, 0, here, :] for d in (4, 3, 2, 1, 0)], axis=0)
            all_scores.append(dots(queries[2, here, :], keys))
        scores = jnp.concatenate(all_scores, axis=0)
        step_q = iota((block, 5 * sub), 0) % sub
        step_k = iota((block, 5 * sub), 1) - 4 * sub
        gap = step_q - step_k
        ok = (gap >= 0) & (gap <= WIN3 // THIRD_DILATION) & (step_k + rank * sub >= 0)
        scores = jnp.where(ok, scores * scale, -jnp.inf)
        top2 = jnp.max(scores, axis=-1, keepdims=True)
        weight = jnp.exp(scores - top2)
        sum2 = jnp.sum(weight, axis=-1, keepdims=True)
        weight = weight.astype(jnp.bfloat16)
        got = []
        for b in range(4):
            here = pl.ds(pl.multiple_of(begin + b * sub, sub), sub)
            vals = jnp.concatenate([far2[d, 1, here, :] for d in (4, 3, 2, 1, 0)], axis=0)
            got.append(jnp.dot(weight[b * sub : (b + 1) * sub], vals, preferred_element_type=jnp.float32))
        got2 = jnp.concatenate(got, axis=0)
        top = jnp.maximum(jnp.maximum(top0, top1), top2)
        f0, f1, f2 = jnp.exp(top0 - top), jnp.exp(top1 - top), jnp.exp(top2 - top)
        total = f0 * sum0 + f1 * sum1 + f2 * sum2
        both = (f0 * got0 + f1 * got1 + f2 * got2) / total
        mine[0, rows, :] = both.astype(jnp.bfloat16)
        return carry

    lax.fori_loop(0, SECOND_DILATION, attend, 0)

    t = iota((tok_rows, tok_rows), 0)
    p = row_time(iota((tok_rows, tok_rows), 1))
    mine[1] = jnp.dot(
        jnp.where(p == t, 1.0, 0.0).astype(jnp.bfloat16), mine[0], preferred_element_type=jnp.float32
    ).astype(jnp.bfloat16)
    head = 2 * x + y
    quarter = tok_rows // 4

    def deal(k):
        return send(mine.at[1, pl.ds(k * quarter, quarter), :], heads_in.at[head], head_s.at[k], head_r.at[head], (2 * z + c, k))

    def deal_self(k):
        return pltpu.make_async_copy(mine.at[1, pl.ds(k * quarter, quarter), :], heads_in.at[head], head_r.at[head])

    for k in range(4):
        self_here = (y == c) & (tp == k)
        pl.when(self_here)(lambda k=k: deal_self(k).start())
        pl.when(jnp.logical_not(self_here))(lambda k=k: deal(k).start())

    o_x().wait()
    o_c().start()
    o_c().wait()
    for h in range(4):
        pltpu.make_async_copy(heads_in.at[h], heads_in.at[h], head_r.at[h]).wait()
    for zz in range(nz):
        for yy in range(2):
            acc = None
            for h in range(4):
                one = jnp.dot(heads_in[h], out_rows[h % 2, h // 2, yy, zz], preferred_element_type=jnp.float32)
                acc = one if acc is None else acc + one
            width = w_out.shape[1]
            s = 2 * zz + yy
            out[:, s * width : (s + 1) * width] = acc.astype(jnp.bfloat16)

    for k in range(4):
        self_here = (y == c) & (tp == k)
        pl.when(jnp.logical_not(self_here))(lambda k=k: deal(k).wait_send())

    @pl.when(jnp.logical_not(stays))
    def _():
        for a in range(3):
            swapped(a).wait_send()
        tok_swapped().wait_send()

    for a in range(4):
        for zz in range(nz):
            pl.when(has_up & (zz <= z))(lambda a=a, zz=zz: go(a, zz, "up").wait_send())
            pl.when(has_down & (zz >= z))(lambda a=a, zz=zz: go(a, zz, "down").wait_send())
            if a < 3:
                go(a, zz, "side").wait_send()
    pl.when(has_up)(lambda: far(0, 0, 2, above).wait_send())
    pl.when(c == 0)(lambda: far(1, 0, 1, side).wait_send())
    pl.when((c == 0) | has_up)(lambda: near(side).wait_send())
    pl.when(has_down & has_up)(lambda: far(2, 2, 4, above).wait_send())
    pl.when(has_down)(lambda: far(3, 2, 3, side).wait_send())
    pl.when((z >= 2) & (c == 1))(lambda: far(4, 4, 3, side).wait_send())


def fits_kernel(n_sp, n_tp, tokens, w_query, w_out):
    tok_rows, depth = tokens.shape
    return (
        n_sp % 2 == 0
        and n_tp == 4
        and w_query.shape[1] == GROUPS * DH
        and w_out.shape[0] == DH
        and w_out.shape[1] % 128 == 0
        and w_query.shape[0] % 16 == 0
        and tok_rows == WIN2
        and 4 * tok_rows == WIN3
        and 4 * WIN1 == tok_rows
    )


def one_kernel(n_sp, tokens, w_query, w_key, w_value, w_out):
    nz = n_sp // 2
    tok_rows, depth = tokens.shape
    cols = w_query.shape[1]
    half = jnp.arange(0, DH, 2, dtype=jnp.float32) / DH
    freq = 1.0 / ROPE_BASE ** half
    freq = jnp.concatenate([freq, freq]).reshape(1, DH)
    bf, dma = jnp.bfloat16, pltpu.SemaphoreType.DMA
    return pl.pallas_call(
        functools.partial(layer_kernel, nz),
        out_shape=jax.ShapeDtypeStruct((tok_rows // 4, w_out.shape[1] * n_sp), bf),
        in_specs=[pl.BlockSpec(memory_space=pltpu.VMEM)] * 6,
        out_specs=pl.BlockSpec(memory_space=pltpu.VMEM),
        scratch_shapes=[
            pltpu.VMEM((3, depth, cols), bf),
            pltpu.VMEM((tok_rows, depth), bf),
            pltpu.VMEM((tok_rows, depth), bf),
            pltpu.VMEM((tok_rows, DH), jnp.float32),
            pltpu.VMEM((tok_rows, DH), jnp.float32),
            pltpu.VMEM((GROUPS, tok_rows, DH), bf),
            pltpu.VMEM((2, tok_rows, DH), bf),
            pltpu.VMEM((2, tok_rows + WIN1, DH), bf),
            pltpu.VMEM((2, tok_rows + WIN1, DH), bf),
            pltpu.VMEM((5, 2, tok_rows, DH), bf),
            pltpu.VMEM((2, 2, 2, nz, *w_out.shape), bf),
            pltpu.VMEM((2, tok_rows, DH), bf),
            pltpu.VMEM((4, tok_rows // 4, DH), bf),
            dma((4,)), dma, dma((3, n_sp)),
            dma((4, nz)), dma((4, nz)), dma((3, nz)),
            dma((nz,)), dma((3,)), dma((3,)),
            dma((5,)), dma((5,)), dma, dma,
            dma((4,)), dma((4,)),
        ],
        compiler_params=pltpu.CompilerParams(
            collective_id=0, has_side_effects=True, vmem_limit_bytes=60000 * 1024
        ),
    )(tokens, w_key, w_value, w_query, w_out, freq)


def on_mesh(n_sp, n_tp, *operands):
    tokens, w_query, _, _, w_out = operands
    if fits_kernel(n_sp, n_tp, tokens, w_query, w_out):
        return one_kernel(n_sp, *operands)
    return on_device(*operands)


def solution(mesh):
    placed = (P("sp", None), P("sp", "tp"), P("sp", "tp"), P("sp", "tp"), P("tp", "sp"))
    body = functools.partial(on_mesh, mesh.shape["sp"], mesh.shape["tp"])
    return jax.shard_map(
        body, mesh=mesh, in_specs=placed, out_specs=P(("sp", "tp"), None), check_vma=False
    )
```

```python
import functools
import math

import jax
import jax.numpy as jnp
import numpy as np
from jax import lax
from jax.experimental import pallas as pl
from jax.experimental.pallas import tpu as pltpu
from jax.sharding import PartitionSpec as P

GROUPS = 3
DH = 128
WIN1 = 128
WIN2 = 512
WIN3 = 2048
SECOND_DILATION = 4
THIRD_DILATION = 16


ROPE_BASE = 500000.0


def from_behind(block, axis, distance):
    devices = range(lax.axis_size(axis))
    route = [(i - distance, i) for i in devices if i - distance in devices]
    return lax.ppermute(block, axis, route)


def rotate(projected, offset):
    tok_rows = projected.shape[0]
    head_size = projected.shape[-1]
    half_size = head_size // 2
    positions = (offset + jnp.arange(tok_rows, dtype=jnp.int32)).astype(jnp.float32)
    frequency = 1.0 / ROPE_BASE ** (jnp.arange(0, head_size, 2, dtype=jnp.float32) / head_size)
    angles = (positions[:, None] * frequency[None, :]).reshape(tok_rows, 1, 1, half_size)
    cosine = jnp.cos(angles)
    sine_part = jnp.sin(angles)
    first_half = projected[..., :half_size]
    second_half = projected[..., half_size:]
    return jnp.concatenate(
        [
            first_half * cosine - second_half * sine_part,
            second_half * cosine + first_half * sine_part,
        ],
        axis=-1,
    )


def window_attend(query_part, buffer, steps, stride, offset):
    tok_rows, heads_here, head_size = query_part.shape
    sub_rows = tok_rows // stride
    key_rows = buffer.shape[1] // stride
    query_sub = query_part.reshape(sub_rows, stride, heads_here, head_size).transpose(1, 2, 0, 3)
    pair_sub = buffer.reshape(2, key_rows, stride, heads_here, head_size).transpose(0, 2, 3, 1, 4)
    block_rows = math.gcd(sub_rows, steps) if sub_rows > steps else sub_rows
    block_list = sub_rows // block_rows
    query_blocks = query_sub.reshape(stride, heads_here, block_list, block_rows, head_size)
    key_blocks = jnp.stack(
        [
            pair_sub[:, :, :, index * block_rows : index * block_rows + block_rows + steps]
            for index in range(block_list)
        ],
        axis=3,
    )
    scores = jnp.einsum(
        "zhnqe,zhnke->zhnqk", query_blocks, key_blocks[0], preferred_element_type=jnp.float32
    ) * head_size ** (-0.5)
    query_index = (jnp.arange(block_list, dtype=jnp.int32) * block_rows)[
        :, None, None
    ] + jnp.arange(block_rows, dtype=jnp.int32)[None, :, None]
    key_index = (jnp.arange(block_list, dtype=jnp.int32) * block_rows)[:, None, None] + jnp.arange(
        block_rows + steps, dtype=jnp.int32
    )[None, None, :]
    spacing = query_index + steps - key_index
    residue = jnp.arange(stride, dtype=jnp.int32)[:, None, None, None]
    key_position = offset + (key_index[None] - steps) * stride + residue
    allowed = (spacing[None] >= 0) & (spacing[None] <= steps) & (key_position >= 0)
    scores = jnp.where(allowed[:, None], scores, -jnp.inf)
    row_max = jnp.max(scores, axis=-1)
    exponent = jnp.exp(scores - row_max[..., None])
    totals = jnp.sum(exponent, axis=-1)
    probs = (exponent / totals[..., None]).astype(jnp.bfloat16)
    mixed = jnp.einsum(
        "zhnqk,zhnke->zhnqe", probs, key_blocks[1], preferred_element_type=jnp.float32
    )
    mixed = mixed.reshape(stride, heads_here, sub_rows, head_size).transpose(2, 0, 1, 3)
    log_total = (row_max + jnp.log(totals)).reshape(stride, heads_here, sub_rows).transpose(2, 0, 1)
    return (mixed.reshape(tok_rows, heads_here, head_size), log_total.reshape(tok_rows, heads_here))


def reach_back(key_value, distance_max):
    tok_rows = key_value.shape[1]
    gathered = key_value
    pieces_held = 1
    while pieces_held < distance_max + 1:
        slice_share = min(pieces_held, distance_max + 1 - pieces_held)
        arrived = from_behind(
            gathered[:, gathered.shape[1] - slice_share * tok_rows :], "sp", pieces_held
        )
        gathered = jnp.concatenate([arrived, gathered], axis=1)
        pieces_held = pieces_held + slice_share
    return gathered


def on_device(tokens, w_query, w_key, w_value, w_out):
    tok_rows = tokens.shape[0]
    heads_here = w_out.shape[0] // DH
    offset = lax.axis_index("sp") * tok_rows
    weight_parts = (
        lax.all_gather(w_query, "sp", axis=0, tiled=True),
        lax.all_gather(w_key, "sp", axis=0, tiled=True),
        lax.all_gather(w_value, "sp", axis=0, tiled=True),
    )
    query_raw, key_raw, value_raw = tuple(
        (
            jnp.dot(tokens, weight_rows, preferred_element_type=jnp.float32)
            for weight_rows in weight_parts
        )
    )
    head_shape = (tok_rows, heads_here, GROUPS, DH)
    queries = rotate(query_raw.reshape(head_shape), offset).astype(jnp.bfloat16)
    keys_all = rotate(key_raw.reshape(head_shape), offset).astype(jnp.bfloat16)
    values_all = value_raw.astype(jnp.bfloat16).reshape(head_shape)
    windows = (WIN1, WIN2, WIN3)
    step_sizes = (1, SECOND_DILATION, THIRD_DILATION)
    outputs = []
    log_totals = []
    for group_index in range(GROUPS):
        key_value = jnp.stack([keys_all[:, :, group_index], values_all[:, :, group_index]])
        key_value = key_value.reshape(2, tok_rows, heads_here * DH)
        window = windows[group_index]
        if group_index == 0:
            near_rows = from_behind(key_value[:, tok_rows - window :], "sp", 1)
            buffer = jnp.concatenate([near_rows, key_value], axis=1)
        else:
            distance_max = (window + tok_rows - 1) // tok_rows
            buffer = reach_back(key_value, distance_max)
        group_out, log_total = window_attend(
            queries[:, :, group_index],
            buffer,
            window // step_sizes[group_index],
            step_sizes[group_index],
            offset,
        )
        outputs.append(group_out)
        log_totals.append(log_total)
    group_weights = jax.nn.softmax(jnp.stack(log_totals), axis=0)
    merged = jnp.sum(group_weights[..., None] * jnp.stack(outputs), axis=0).astype(jnp.bfloat16)
    merged = merged.reshape(tok_rows, heads_here * DH)
    w_whole = lax.all_gather(w_out, "sp", axis=1, tiled=True)
    return lax.psum_scatter(
        jnp.dot(merged, w_whole, preferred_element_type=jnp.float32).astype(jnp.bfloat16),
        "tp",
        scatter_dimension=0,
        tiled=True,
    )


def layer_kernel(
    nz,
    tokens, w_key, w_value, w_query, w_out, freq, out,
    weights, tok_in, tok_turned, cosine, sine, queries, pair0, send1, near1, far2,
    out_rows, mine, heads_in, got01, top01, sum01,
    swap_s, tok_r, w_r, up_s, down_s, side_s, o_r, o_s, o_r2, far_s, far_r, near_s, near_r, head_s, head_r,
):
    tok_rows, depth = tokens.shape
    k_rows, cols = w_key.shape
    sub = tok_rows // THIRD_DILATION
    sub_log = sub.bit_length() - 1
    block = tok_rows // SECOND_DILATION
    tail = WIN1
    sp, tp = lax.axis_index("sp"), lax.axis_index("tp")
    z, y = sp // 2, sp % 2
    x, c = tp // 2, tp % 2
    rank = 2 * z + c
    side = (sp, 2 * x + 1 - c)
    above = (sp + 2, tp)
    below = (sp - 2, tp)
    partner = (2 * z + 1 - y, 2 * x + 1 - c)
    stays = c == y
    has_up, has_down = z < nz - 1, z > 0

    def send(src, dst, s_sem, r_sem, where):
        return pltpu.make_async_remote_copy(
            src_ref=src, dst_ref=dst, send_sem=s_sem, recv_sem=r_sem,
            device_id=where, device_id_type=pl.DeviceIdType.MESH,
        )

    barrier = pltpu.get_barrier_semaphore()

    def greet(where):
        pl.semaphore_signal(barrier, inc=1, device_id=where, device_id_type=pl.DeviceIdType.MESH)

    for dy in range(2):
        for dx in range(2):
            for dc in range(2):
                if dy + dx + dc:
                    greet((2 * z + (y + dy) % 2, 2 * ((x + dx) % 2) + (c + dc) % 2))
    pl.when(has_up)(lambda: greet(above))
    pl.when(has_down)(lambda: greet(below))
    pl.when(has_up & (c == 1))(lambda: greet((sp + 2, 2 * x)))
    pl.when(has_down & (c == 0))(lambda: greet((sp - 2, 2 * x + 1)))
    greeters = 7 + jnp.where(has_up, 1 + c, 0) + jnp.where(has_down, 2 - c, 0)
    pl.semaphore_wait(barrier, greeters)

    parts = (w_key, w_value, w_query)

    def chunk(a, s):
        return weights.at[a, pl.ds(pl.multiple_of(s * k_rows, k_rows), k_rows), :]

    def o_chunk(zz):
        return out_rows.at[c, x, y, zz]

    def swapped(a):
        there = 2 * z + 1 - c
        return send(parts[a], chunk(a, there), swap_s.at[a], w_r.at[a, there], partner)

    def tok_swapped():
        return send(tokens, tok_in, swap_s.at[3], tok_r, partner)

    def kept(a):
        return pltpu.make_async_copy(parts[a], chunk(a, rank), w_r.at[a, rank])

    def o_kept():
        return pltpu.make_async_copy(w_out, o_chunk(z), o_r.at[z])

    @pl.when(stays)
    def _():
        for a in range(3):
            kept(a).start()

    @pl.when(jnp.logical_not(stays))
    def _():
        swapped(0).start()
        swapped(1).start()
        tok_swapped().start()
        swapped(2).start()

    o_kept().start()

    def go(a, zz, kind):
        s = 2 * zz + c
        ref = chunk(a, s) if a < 3 else o_chunk(zz)
        r_sem = w_r.at[a, s] if a < 3 else o_r.at[zz]
        s_sem = {"up": up_s, "down": down_s, "side": side_s}[kind].at[a, zz]
        return send(ref, ref, s_sem, r_sem, {"up": above, "down": below, "side": side}[kind])

    def own(a):
        if a < 3:
            pl.when(stays)(lambda: kept(a).wait())
            pl.when(jnp.logical_not(stays))(lambda: go(a, z, "side").wait_recv())
        else:
            o_kept().wait()
        pl.when(has_up)(lambda: go(a, z, "up").start())
        pl.when(has_down)(lambda: go(a, z, "down").start())
        if a < 3:
            go(a, z, "side").start()

    def relay(a, d):
        @pl.when(z - d >= 0)
        def _():
            go(a, z - d, "up").wait_recv()
            pl.when(has_up)(lambda: go(a, z - d, "up").start())
            if a < 3:
                go(a, z - d, "side").start()

        @pl.when(z + d < nz)
        def _():
            go(a, z + d, "down").wait_recv()
            pl.when(has_down)(lambda: go(a, z + d, "down").start())
            if a < 3:
                go(a, z + d, "side").start()

    def others(a):
        for zz in range(nz):
            s = 2 * zz + 1 - c
            send(chunk(a, s), chunk(a, s), side_s.at[a, zz], w_r.at[a, s], side).wait_recv()

    def row_time(p):
        b, i = p >> sub_log, p & (sub - 1)
        return THIRD_DILATION * i + (b >> 2) + SECOND_DILATION * (b & 3)

    def tail_time(u):
        per = tail // THIRD_DILATION
        b, i = u >> (per.bit_length() - 1), u & (per - 1)
        return THIRD_DILATION * (sub - per + i) + (b >> 2) + SECOND_DILATION * (b & 3) - tok_rows

    own(0)
    own(1)

    def angles(index, carry):
        rows = pl.ds(pl.multiple_of(index * block, block), block)
        p = lax.broadcasted_iota(jnp.int32, (block, DH), 0) + index * block
        angle = (row_time(p) + rank * tok_rows).astype(jnp.float32) * freq[...]
        lane = lax.broadcasted_iota(jnp.int32, (block, DH), 1)
        cosine[rows, :] = jnp.cos(angle)
        turned = jnp.sin(angle)
        sine[rows, :] = jnp.where(lane < DH // 2, -turned, turned)
        return carry

    lax.fori_loop(0, SECOND_DILATION, angles, 0)

    def relay_all(a, following):
        for d in range(1, nz):
            if d == nz - 1 and following is not None:
                own(following)
            relay(a, d)

    def order(source):
        p = row_time(lax.broadcasted_iota(jnp.int32, (tok_rows, tok_rows), 0))
        t = lax.broadcasted_iota(jnp.int32, (tok_rows, tok_rows), 1)
        pick = jnp.where(p == t, 1.0, 0.0).astype(jnp.bfloat16)

        def piece(index, carry):
            at = pl.ds(pl.multiple_of(index * 256, 256), 256)
            tok_turned[:, at] = jnp.dot(
                pick, source[:, at], preferred_element_type=jnp.float32
            ).astype(jnp.bfloat16)
            return carry

        lax.fori_loop(0, depth // 256, piece, 0)

    pl.when(stays)(lambda: order(tokens))

    def o_y():
        return send(out_rows.at[c, x, y], out_rows.at[c, x, y], o_s.at[0], o_r2.at[0], (2 * z + 1 - y, tp))

    def o_x():
        return send(out_rows.at[c, x], out_rows.at[c, x], o_s.at[1], o_r2.at[1], (sp, 2 * (1 - x) + c))

    def o_c():
        return send(out_rows.at[c], out_rows.at[c], o_s.at[2], o_r2.at[2], side)

    relay_all(0, 3)
    relay_all(3, None)
    o_y().start()
    relay_all(1, 2)
    relay(2, 1)

    @pl.when(jnp.logical_not(stays))
    def _():
        tok_swapped().wait_recv()
        order(tok_in)

    def project(a, store):
        def piece(index, carry):
            rows = pl.ds(pl.multiple_of(index * block, block), block)
            raw = jnp.dot(tok_turned[rows, :], weights[a], preferred_element_type=jnp.float32)
            for g in range(GROUPS):
                part = raw[:, g * DH : (g + 1) * DH]
                if a != 1:
                    part = part * cosine[rows, :] + pltpu.roll(part, DH // 2, 1) * sine[rows, :]
                store(index, rows, g, part)
            return carry

        lax.fori_loop(0, SECOND_DILATION, piece, 0)

    def keep_pair(which):
        def store(index, rows, g, part):
            if g == 2:
                far2[0, which, rows, :] = part.astype(jnp.bfloat16)
            elif g == 1:
                send1[which, rows, :] = part.astype(jnp.bfloat16)
            else:
                pair0[which, rows, :] = part.astype(jnp.bfloat16)
                per = tail // THIRD_DILATION
                last = jnp.concatenate(
                    [part[b * sub + sub - per : (b + 1) * sub] for b in range(4)], axis=0
                )
                at = pl.ds(pl.multiple_of(tok_rows + index * 4 * per, 4 * per), 4 * per)
                send1[which, at, :] = last.astype(jnp.bfloat16)

        return store

    others(0)
    project(0, keep_pair(0))
    others(1)
    project(1, keep_pair(1))

    def far(index, src, dst, where):
        return send(far2.at[src], far2.at[dst], far_s.at[index], far_r.at[dst], where)

    def near(where):
        return send(send1, near1, near_s, near_r, where)

    up_other = (sp + 2, 2 * x)
    pl.when(has_up)(lambda: far(0, 0, 2, above).start())
    pl.when(c == 0)(lambda: far(1, 0, 1, side).start())
    pl.when(c == 0)(lambda: near(side).start())
    pl.when(has_up & (c == 1))(lambda: near(up_other).start())

    for d in range(1, 5):
        @pl.when(rank < d)
        def _(d=d):
            far2[d] = jnp.zeros(far2.shape[1:], far2.dtype)

    @pl.when(rank < 1)
    def _():
        near1[...] = jnp.zeros(near1.shape, near1.dtype)

    for d in range(2, nz):
        relay(2, d)
    @pl.when(has_down)
    def _():
        far(0, 0, 2, above).wait_recv()
        pl.when(has_up)(lambda: far(2, 2, 4, above).start())
        pl.when(c == 0)(lambda: far(3, 2, 3, side).start())
        pl.when(c == 1)(lambda: far(3, 2, 1, side).start())

    o_y().wait()
    o_x().start()
    others(2)

    def keep_query(index, rows, g, part):
        queries[g, rows, :] = part.astype(jnp.bfloat16)

    project(2, keep_query)

    scale = DH ** (-0.5)
    far_off = 1 << 24

    def dots(q, k):
        return lax.dot_general(q, k, (((1,), (1,)), ((), ())), preferred_element_type=jnp.float32)

    def iota(shape, axis):
        return lax.broadcasted_iota(jnp.int32, shape, axis)

    def soft(scores, time_q, time_k, reach, first):
        gap = time_q - jnp.where(time_k >= first, time_k, far_off)
        scores = jnp.where((gap >= 0) & (gap <= reach), scores * scale, -jnp.inf)
        top = jnp.max(scores, axis=-1, keepdims=True)
        weight = jnp.exp(scores - top)
        return top, jnp.sum(weight, axis=-1, keepdims=True), weight.astype(jnp.bfloat16)

    def near_groups(index, carry):
        begin = index * block
        rows = pl.ds(pl.multiple_of(begin, block), block)
        q = queries[0, rows, :]
        tails = pl.ds(tok_rows, tail)
        scores = jnp.concatenate([dots(q, near1[0, tails, :]), dots(q, pair0[0])], axis=1)
        lane = iota((1, tail + tok_rows), 1)
        time_k = jnp.where(lane < tail, tail_time(lane & (tail - 1)), row_time(lane - tail))
        time_q = row_time(iota((block, 1), 0) + begin)
        top0, sum0, weight = soft(scores, time_q, time_k, WIN1, -rank * tok_rows)
        got0 = jnp.dot(weight[:, :tail], near1[1, tails, :], preferred_element_type=jnp.float32)
        got0 += jnp.dot(weight[:, tail:], pair0[1], preferred_element_type=jnp.float32)
        q = queries[1, rows, :]
        scores = jnp.concatenate([dots(q, near1[0, rows, :]), dots(q, send1[0, rows, :])], axis=1)

        def step_of(place):
            return 4 * (place & (sub - 1)) + (place >> sub_log)

        lane = iota((1, 2 * block), 1)
        step_k = step_of(lane & (block - 1)) + jnp.where(lane < block, -block, 0)
        top1, sum1, weight = soft(
            scores, step_of(iota((block, 1), 0)), step_k, WIN2 // SECOND_DILATION, -rank * block
        )
        got1 = jnp.dot(weight[:, :block], near1[1, rows, :], preferred_element_type=jnp.float32)
        got1 += jnp.dot(weight[:, block:], send1[1, rows, :], preferred_element_type=jnp.float32)
        top = jnp.maximum(top0, top1)
        f0, f1 = jnp.exp(top0 - top), jnp.exp(top1 - top)
        got01[rows, :] = f0 * got0 + f1 * got1
        top01[rows, :] = top
        sum01[rows, :] = f0 * sum0 + f1 * sum1
        return carry

    def far_group(index, carry):
        begin = index * block
        rows = pl.ds(pl.multiple_of(begin, block), block)
        all_scores = []
        for b in range(4):
            here = pl.ds(pl.multiple_of(begin + b * sub, sub), sub)
            keys = jnp.concatenate([far2[d, 0, here, :] for d in (4, 3, 2, 1, 0)], axis=0)
            all_scores.append(dots(queries[2, here, :], keys))
        scores = jnp.concatenate(all_scores, axis=0)
        step_q = iota((block, 1), 0) & (sub - 1)
        step_k = iota((1, 5 * sub), 1) - 4 * sub
        top2, sum2, weight = soft(scores, step_q, step_k, WIN3 // THIRD_DILATION, -rank * sub)
        got = []
        for b in range(4):
            here = pl.ds(pl.multiple_of(begin + b * sub, sub), sub)
            vals = jnp.concatenate([far2[d, 1, here, :] for d in (4, 3, 2, 1, 0)], axis=0)
            got.append(jnp.dot(weight[b * sub : (b + 1) * sub], vals, preferred_element_type=jnp.float32))
        got2 = jnp.concatenate(got, axis=0)
        top1 = top01[rows, :]
        top = jnp.maximum(top1, top2)
        f1, f2 = jnp.exp(top1 - top), jnp.exp(top2 - top)
        total = f1 * sum01[rows, :] + f2 * sum2
        mine[0, rows, :] = ((f1 * got01[rows, :] + f2 * got2) / total).astype(jnp.bfloat16)
        return carry

    pl.when(rank >= 1)(lambda: near(side).wait_recv())
    lax.fori_loop(0, SECOND_DILATION, near_groups, 0)
    o_x().wait()
    o_c().start()

    @pl.when(z >= 2)
    def _():
        far(2, 2, 4, above).wait_recv()
        pl.when(c == 1)(lambda: far(4, 4, 3, side).start())

    pl.when(rank >= 1)(lambda: far(1, 0, 1, side).wait_recv())
    pl.when(rank >= 3)(lambda: far(4, 4, 3, side).wait_recv())
    lax.fori_loop(0, SECOND_DILATION, far_group, 0)

    t = iota((tok_rows, tok_rows), 0)
    p = row_time(iota((tok_rows, tok_rows), 1))
    mine[1] = jnp.dot(
        jnp.where(p == t, 1.0, 0.0).astype(jnp.bfloat16), mine[0], preferred_element_type=jnp.float32
    ).astype(jnp.bfloat16)
    head = 2 * x + y
    quarter = tok_rows // 4

    def deal(k):
        return send(mine.at[1, pl.ds(k * quarter, quarter), :], heads_in.at[head], head_s.at[k], head_r.at[head], (2 * z + c, k))

    def deal_self(k):
        return pltpu.make_async_copy(mine.at[1, pl.ds(k * quarter, quarter), :], heads_in.at[head], head_r.at[head])

    for k in range(4):
        self_here = (y == c) & (tp == k)
        pl.when(self_here)(lambda k=k: deal_self(k).start())
        pl.when(jnp.logical_not(self_here))(lambda k=k: deal(k).start())

    o_c().wait()
    for h in range(4):
        pltpu.make_async_copy(heads_in.at[h], heads_in.at[h], head_r.at[h]).wait()
    for zz in range(nz):
        for yy in range(2):
            acc = None
            for h in range(4):
                one = jnp.dot(heads_in[h], out_rows[h % 2, h // 2, yy, zz], preferred_element_type=jnp.float32)
                acc = one if acc is None else acc + one
            width = w_out.shape[1]
            s = 2 * zz + yy
            out[:, s * width : (s + 1) * width] = acc.astype(jnp.bfloat16)

    for k in range(4):
        self_here = (y == c) & (tp == k)
        pl.when(jnp.logical_not(self_here))(lambda k=k: deal(k).wait_send())

    @pl.when(jnp.logical_not(stays))
    def _():
        for a in range(3):
            swapped(a).wait_send()
        tok_swapped().wait_send()

    for a in range(4):
        for zz in range(nz):
            pl.when(has_up & (zz <= z))(lambda a=a, zz=zz: go(a, zz, "up").wait_send())
            pl.when(has_down & (zz >= z))(lambda a=a, zz=zz: go(a, zz, "down").wait_send())
            if a < 3:
                go(a, zz, "side").wait_send()
    pl.when(has_up)(lambda: far(0, 0, 2, above).wait_send())
    pl.when(c == 0)(lambda: far(1, 0, 1, side).wait_send())
    pl.when((c == 0) | has_up)(lambda: near(side).wait_send())
    pl.when(has_down & has_up)(lambda: far(2, 2, 4, above).wait_send())
    pl.when(has_down)(lambda: far(3, 2, 3, side).wait_send())
    pl.when((z >= 2) & (c == 1))(lambda: far(4, 4, 3, side).wait_send())


def fits_kernel(n_sp, n_tp, tokens, w_query, w_out):
    tok_rows, depth = tokens.shape
    return (
        n_sp % 2 == 0
        and n_tp == 4
        and w_query.shape[1] == GROUPS * DH
        and w_out.shape[0] == DH
        and w_out.shape[1] % 128 == 0
        and w_query.shape[0] % 16 == 0
        and tok_rows == WIN2
        and 4 * tok_rows == WIN3
        and 4 * WIN1 == tok_rows
    )


def one_kernel(n_sp, tokens, w_query, w_key, w_value, w_out):
    nz = n_sp // 2
    tok_rows, depth = tokens.shape
    cols = w_query.shape[1]
    half = 1.0 / ROPE_BASE ** (np.arange(0, DH, 2) / DH)
    freq = jnp.asarray(np.concatenate([half, half]).reshape(1, DH), jnp.float32)
    bf, dma = jnp.bfloat16, pltpu.SemaphoreType.DMA
    return pl.pallas_call(
        functools.partial(layer_kernel, nz),
        out_shape=jax.ShapeDtypeStruct((tok_rows // 4, w_out.shape[1] * n_sp), bf),
        in_specs=[pl.BlockSpec(memory_space=pltpu.VMEM)] * 6,
        out_specs=pl.BlockSpec(memory_space=pltpu.VMEM),
        scratch_shapes=[
            pltpu.VMEM((3, depth, cols), bf),
            pltpu.VMEM((tok_rows, depth), bf),
            pltpu.VMEM((tok_rows, depth), bf),
            pltpu.VMEM((tok_rows, DH), jnp.float32),
            pltpu.VMEM((tok_rows, DH), jnp.float32),
            pltpu.VMEM((GROUPS, tok_rows, DH), bf),
            pltpu.VMEM((2, tok_rows, DH), bf),
            pltpu.VMEM((2, tok_rows + WIN1, DH), bf),
            pltpu.VMEM((2, tok_rows + WIN1, DH), bf),
            pltpu.VMEM((5, 2, tok_rows, DH), bf),
            pltpu.VMEM((2, 2, 2, nz, *w_out.shape), bf),
            pltpu.VMEM((2, tok_rows, DH), bf),
            pltpu.VMEM((4, tok_rows // 4, DH), bf),
            pltpu.VMEM((tok_rows, DH), jnp.float32),
            pltpu.VMEM((tok_rows, 1), jnp.float32),
            pltpu.VMEM((tok_rows, 1), jnp.float32),
            dma((4,)), dma, dma((3, n_sp)),
            dma((4, nz)), dma((4, nz)), dma((3, nz)),
            dma((nz,)), dma((3,)), dma((3,)),
            dma((5,)), dma((5,)), dma, dma,
            dma((4,)), dma((4,)),
        ],
        compiler_params=pltpu.CompilerParams(
            collective_id=0, has_side_effects=True, vmem_limit_bytes=32 * 1024 * 1024
        ),
    )(tokens, w_key, w_value, w_query, w_out, freq)


def on_mesh(n_sp, n_tp, *operands):
    tokens, w_query, _, _, w_out = operands
    if fits_kernel(n_sp, n_tp, tokens, w_query, w_out):
        return one_kernel(n_sp, *operands)
    return on_device(*operands)


def solution(mesh):
    placed = (P("sp", None), P("sp", "tp"), P("sp", "tp"), P("sp", "tp"), P("tp", "sp"))
    body = functools.partial(on_mesh, mesh.shape["sp"], mesh.shape["tp"])
    return jax.shard_map(
        body, mesh=mesh, in_specs=placed, out_specs=P(("sp", "tp"), None), check_vma=False
    )
```

```python
import functools
import math

import jax
import jax.numpy as jnp
from jax import lax
from jax.experimental import pallas as pl
from jax.experimental.pallas import tpu as pltpu
from jax.sharding import PartitionSpec as P

GROUPS = 3
DH = 128
WIN1 = 128
WIN2 = 512
WIN3 = 2048
SECOND_DILATION = 4
THIRD_DILATION = 16


ROPE_BASE = 500000.0


def from_behind(block, axis, distance):
    devices = range(lax.axis_size(axis))
    route = [(i - distance, i) for i in devices if i - distance in devices]
    return lax.ppermute(block, axis, route)


def rotate(projected, offset):
    tok_rows = projected.shape[0]
    head_size = projected.shape[-1]
    half_size = head_size // 2
    positions = (offset + jnp.arange(tok_rows, dtype=jnp.int32)).astype(jnp.float32)
    frequency = 1.0 / ROPE_BASE ** (jnp.arange(0, head_size, 2, dtype=jnp.float32) / head_size)
    angles = (positions[:, None] * frequency[None, :]).reshape(tok_rows, 1, 1, half_size)
    cosine = jnp.cos(angles)
    sine_part = jnp.sin(angles)
    first_half = projected[..., :half_size]
    second_half = projected[..., half_size:]
    return jnp.concatenate(
        [
            first_half * cosine - second_half * sine_part,
            second_half * cosine + first_half * sine_part,
        ],
        axis=-1,
    )


def window_attend(query_part, buffer, steps, stride, offset):
    tok_rows, heads_here, head_size = query_part.shape
    sub_rows = tok_rows // stride
    key_rows = buffer.shape[1] // stride
    query_sub = query_part.reshape(sub_rows, stride, heads_here, head_size).transpose(1, 2, 0, 3)
    pair_sub = buffer.reshape(2, key_rows, stride, heads_here, head_size).transpose(0, 2, 3, 1, 4)
    block_rows = math.gcd(sub_rows, steps) if sub_rows > steps else sub_rows
    block_list = sub_rows // block_rows
    query_blocks = query_sub.reshape(stride, heads_here, block_list, block_rows, head_size)
    key_blocks = jnp.stack(
        [
            pair_sub[:, :, :, index * block_rows : index * block_rows + block_rows + steps]
            for index in range(block_list)
        ],
        axis=3,
    )
    scores = jnp.einsum(
        "zhnqe,zhnke->zhnqk", query_blocks, key_blocks[0], preferred_element_type=jnp.float32
    ) * head_size ** (-0.5)
    query_index = (jnp.arange(block_list, dtype=jnp.int32) * block_rows)[
        :, None, None
    ] + jnp.arange(block_rows, dtype=jnp.int32)[None, :, None]
    key_index = (jnp.arange(block_list, dtype=jnp.int32) * block_rows)[:, None, None] + jnp.arange(
        block_rows + steps, dtype=jnp.int32
    )[None, None, :]
    spacing = query_index + steps - key_index
    residue = jnp.arange(stride, dtype=jnp.int32)[:, None, None, None]
    key_position = offset + (key_index[None] - steps) * stride + residue
    allowed = (spacing[None] >= 0) & (spacing[None] <= steps) & (key_position >= 0)
    scores = jnp.where(allowed[:, None], scores, -jnp.inf)
    row_max = jnp.max(scores, axis=-1)
    exponent = jnp.exp(scores - row_max[..., None])
    totals = jnp.sum(exponent, axis=-1)
    probs = (exponent / totals[..., None]).astype(jnp.bfloat16)
    mixed = jnp.einsum(
        "zhnqk,zhnke->zhnqe", probs, key_blocks[1], preferred_element_type=jnp.float32
    )
    mixed = mixed.reshape(stride, heads_here, sub_rows, head_size).transpose(2, 0, 1, 3)
    log_total = (row_max + jnp.log(totals)).reshape(stride, heads_here, sub_rows).transpose(2, 0, 1)
    return (mixed.reshape(tok_rows, heads_here, head_size), log_total.reshape(tok_rows, heads_here))


def reach_back(key_value, distance_max):
    tok_rows = key_value.shape[1]
    gathered = key_value
    pieces_held = 1
    while pieces_held < distance_max + 1:
        slice_share = min(pieces_held, distance_max + 1 - pieces_held)
        arrived = from_behind(
            gathered[:, gathered.shape[1] - slice_share * tok_rows :], "sp", pieces_held
        )
        gathered = jnp.concatenate([arrived, gathered], axis=1)
        pieces_held = pieces_held + slice_share
    return gathered


def on_device(tokens, w_query, w_key, w_value, w_out):
    tok_rows = tokens.shape[0]
    heads_here = w_out.shape[0] // DH
    offset = lax.axis_index("sp") * tok_rows
    weight_parts = (
        lax.all_gather(w_query, "sp", axis=0, tiled=True),
        lax.all_gather(w_key, "sp", axis=0, tiled=True),
        lax.all_gather(w_value, "sp", axis=0, tiled=True),
    )
    query_raw, key_raw, value_raw = tuple(
        (
            jnp.dot(tokens, weight_rows, preferred_element_type=jnp.float32)
            for weight_rows in weight_parts
        )
    )
    head_shape = (tok_rows, heads_here, GROUPS, DH)
    queries = rotate(query_raw.reshape(head_shape), offset).astype(jnp.bfloat16)
    keys_all = rotate(key_raw.reshape(head_shape), offset).astype(jnp.bfloat16)
    values_all = value_raw.astype(jnp.bfloat16).reshape(head_shape)
    windows = (WIN1, WIN2, WIN3)
    step_sizes = (1, SECOND_DILATION, THIRD_DILATION)
    outputs = []
    log_totals = []
    for group_index in range(GROUPS):
        key_value = jnp.stack([keys_all[:, :, group_index], values_all[:, :, group_index]])
        key_value = key_value.reshape(2, tok_rows, heads_here * DH)
        window = windows[group_index]
        if group_index == 0:
            near_rows = from_behind(key_value[:, tok_rows - window :], "sp", 1)
            buffer = jnp.concatenate([near_rows, key_value], axis=1)
        else:
            distance_max = (window + tok_rows - 1) // tok_rows
            buffer = reach_back(key_value, distance_max)
        group_out, log_total = window_attend(
            queries[:, :, group_index],
            buffer,
            window // step_sizes[group_index],
            step_sizes[group_index],
            offset,
        )
        outputs.append(group_out)
        log_totals.append(log_total)
    group_weights = jax.nn.softmax(jnp.stack(log_totals), axis=0)
    merged = jnp.sum(group_weights[..., None] * jnp.stack(outputs), axis=0).astype(jnp.bfloat16)
    merged = merged.reshape(tok_rows, heads_here * DH)
    w_whole = lax.all_gather(w_out, "sp", axis=1, tiled=True)
    return lax.psum_scatter(
        jnp.dot(merged, w_whole, preferred_element_type=jnp.float32).astype(jnp.bfloat16),
        "tp",
        scatter_dimension=0,
        tiled=True,
    )


def layer_kernel(
    nz,
    tokens, w_key, w_value, w_query, w_out, out,
    weights, tok_in, tok_turned, cosine, sine, queries, pair0, send1, near1, far2,
    out_rows, mine, heads_in, got01, top01, sum01,
    swap_s, tok_r, w_r, up_s, down_s, side_s, o_r, o_s, o_r2, far_s, far_r, near_s, near_r, head_s, head_r,
):
    tok_rows, depth = tokens.shape
    k_rows, cols = w_key.shape
    sub = tok_rows // THIRD_DILATION
    sub_log = sub.bit_length() - 1
    block = tok_rows // SECOND_DILATION
    tail = WIN1
    sp, tp = lax.axis_index("sp"), lax.axis_index("tp")
    z, y = sp // 2, sp % 2
    x, c = tp // 2, tp % 2
    rank = 2 * z + c
    side = (sp, 2 * x + 1 - c)
    above = (sp + 2, tp)
    below = (sp - 2, tp)
    partner = (2 * z + 1 - y, 2 * x + 1 - c)
    stays = c == y
    has_up, has_down = z < nz - 1, z > 0

    def send(src, dst, s_sem, r_sem, where):
        return pltpu.make_async_remote_copy(
            src_ref=src, dst_ref=dst, send_sem=s_sem, recv_sem=r_sem,
            device_id=where, device_id_type=pl.DeviceIdType.MESH,
        )

    parts = (w_key, w_value, w_query)

    def chunk(a, s):
        return weights.at[a, pl.ds(pl.multiple_of(s * k_rows, k_rows), k_rows), :]

    def o_chunk(zz):
        return out_rows.at[c, x, y, zz]

    def swapped(a):
        there = 2 * z + 1 - c
        return send(parts[a], chunk(a, there), swap_s.at[a], w_r.at[a, there], partner)

    def tok_swapped():
        return send(tokens, tok_in, swap_s.at[3], tok_r, partner)

    def kept(a):
        return pltpu.make_async_copy(parts[a], chunk(a, rank), w_r.at[a, rank])

    def o_kept():
        return pltpu.make_async_copy(w_out, o_chunk(z), o_r.at[z])

    def tok_kept():
        return pltpu.make_async_copy(tokens, tok_in, tok_r)

    @pl.when(stays)
    def _():
        for a in range(3):
            kept(a).start()
        tok_kept().start()

    o_kept().start()

    barrier = pltpu.get_barrier_semaphore()

    def greet(where):
        pl.semaphore_signal(barrier, inc=1, device_id=where, device_id_type=pl.DeviceIdType.MESH)

    for dy in range(2):
        for dx in range(2):
            for dc in range(2):
                if dy + dx + dc:
                    greet((2 * z + (y + dy) % 2, 2 * ((x + dx) % 2) + (c + dc) % 2))
    pl.when(has_up)(lambda: greet(above))
    pl.when(has_down)(lambda: greet(below))
    pl.when(has_up & (c == 1))(lambda: greet((sp + 2, 2 * x)))
    pl.when(has_down & (c == 0))(lambda: greet((sp - 2, 2 * x + 1)))
    greeters = 7 + jnp.where(has_up, 1 + c, 0) + jnp.where(has_down, 2 - c, 0)
    pl.semaphore_wait(barrier, greeters)

    @pl.when(jnp.logical_not(stays))
    def _():
        swapped(0).start()
        swapped(1).start()
        tok_swapped().start()
        swapped(2).start()

    def go(a, zz, kind):
        s = 2 * zz + c
        ref = chunk(a, s) if a < 3 else o_chunk(zz)
        r_sem = w_r.at[a, s] if a < 3 else o_r.at[zz]
        s_sem = {"up": up_s, "down": down_s, "side": side_s}[kind].at[a, zz]
        return send(ref, ref, s_sem, r_sem, {"up": above, "down": below, "side": side}[kind])

    def own(a):
        if a < 3:
            pl.when(stays)(lambda: kept(a).wait())
            pl.when(jnp.logical_not(stays))(lambda: go(a, z, "side").wait_recv())
        else:
            o_kept().wait()
        pl.when(has_up)(lambda: go(a, z, "up").start())
        pl.when(has_down)(lambda: go(a, z, "down").start())
        if a < 3:
            go(a, z, "side").start()

    def relay(a, d):
        @pl.when(z - d >= 0)
        def _():
            go(a, z - d, "up").wait_recv()
            pl.when(has_up)(lambda: go(a, z - d, "up").start())
            if a < 3:
                go(a, z - d, "side").start()

        @pl.when(z + d < nz)
        def _():
            go(a, z + d, "down").wait_recv()
            pl.when(has_down)(lambda: go(a, z + d, "down").start())
            if a < 3:
                go(a, z + d, "side").start()

    def others(a):
        for zz in range(nz):
            s = 2 * zz + 1 - c
            send(chunk(a, s), chunk(a, s), side_s.at[a, zz], w_r.at[a, s], side).wait_recv()

    def row_time(p):
        b, i = p >> sub_log, p & (sub - 1)
        return THIRD_DILATION * i + (b >> 2) + SECOND_DILATION * (b & 3)

    def tail_time(u):
        per = tail // THIRD_DILATION
        b, i = u >> (per.bit_length() - 1), u & (per - 1)
        return THIRD_DILATION * (sub - per + i) + (b >> 2) + SECOND_DILATION * (b & 3) - tok_rows

    own(0)
    own(1)

    pair_at = lax.broadcasted_iota(jnp.int32, (1, DH), 1) & (DH // 2 - 1)
    freq = jnp.exp(pair_at.astype(jnp.float32) * (-2.0 * math.log(ROPE_BASE) / DH))

    def angles(index, carry):
        rows = pl.ds(pl.multiple_of(index * block, block), block)
        p = lax.broadcasted_iota(jnp.int32, (block, DH), 0) + index * block
        angle = (row_time(p) + rank * tok_rows).astype(jnp.float32) * freq
        lane = lax.broadcasted_iota(jnp.int32, (block, DH), 1)
        cosine[rows, :] = jnp.cos(angle)
        turned = jnp.sin(angle)
        sine[rows, :] = jnp.where(lane < DH // 2, -turned, turned)
        return carry

    lax.fori_loop(0, SECOND_DILATION, angles, 0)

    def relay_all(a, following):
        for d in range(1, nz):
            if d == nz - 1 and following is not None:
                own(following)
            relay(a, d)

    def order(source):
        p = row_time(lax.broadcasted_iota(jnp.int32, (tok_rows, tok_rows), 0))
        t = lax.broadcasted_iota(jnp.int32, (tok_rows, tok_rows), 1)
        pick = jnp.where(p == t, 1.0, 0.0).astype(jnp.bfloat16)

        def piece(index, carry):
            at = pl.ds(pl.multiple_of(index * 256, 256), 256)
            tok_turned[:, at] = jnp.dot(
                pick, source[:, at], preferred_element_type=jnp.float32
            ).astype(jnp.bfloat16)
            return carry

        lax.fori_loop(0, depth // 256, piece, 0)

    @pl.when(stays)
    def _():
        tok_kept().wait()
        order(tok_in)

    def o_y():
        return send(out_rows.at[c, x, y], out_rows.at[c, x, y], o_s.at[0], o_r2.at[0], (2 * z + 1 - y, tp))

    def o_x():
        return send(out_rows.at[c, x], out_rows.at[c, x], o_s.at[1], o_r2.at[1], (sp, 2 * (1 - x) + c))

    def o_c():
        return send(out_rows.at[c], out_rows.at[c], o_s.at[2], o_r2.at[2], side)

    relay_all(0, 3)
    relay_all(3, None)
    o_y().start()
    relay_all(1, 2)
    relay(2, 1)

    @pl.when(jnp.logical_not(stays))
    def _():
        tok_swapped().wait_recv()
        order(tok_in)

    def project(a, store):
        def piece(index, carry):
            rows = pl.ds(pl.multiple_of(index * block, block), block)
            raw = jnp.dot(tok_turned[rows, :], weights[a], preferred_element_type=jnp.float32)
            for g in range(GROUPS):
                part = raw[:, g * DH : (g + 1) * DH]
                if a != 1:
                    part = part * cosine[rows, :] + pltpu.roll(part, DH // 2, 1) * sine[rows, :]
                store(index, rows, g, part)
            return carry

        lax.fori_loop(0, SECOND_DILATION, piece, 0)

    def keep_pair(which):
        def store(index, rows, g, part):
            if g == 2:
                far2[0, which, rows, :] = part.astype(jnp.bfloat16)
            elif g == 1:
                send1[which, rows, :] = part.astype(jnp.bfloat16)
            else:
                pair0[which, rows, :] = part.astype(jnp.bfloat16)
                per = tail // THIRD_DILATION
                last = jnp.concatenate(
                    [part[b * sub + sub - per : (b + 1) * sub] for b in range(4)], axis=0
                )
                at = pl.ds(pl.multiple_of(tok_rows + index * 4 * per, 4 * per), 4 * per)
                send1[which, at, :] = last.astype(jnp.bfloat16)

        return store

    others(0)
    project(0, keep_pair(0))
    others(1)
    project(1, keep_pair(1))

    def far(index, src, dst, where):
        return send(far2.at[src], far2.at[dst], far_s.at[index], far_r.at[dst], where)

    def near(where):
        return send(send1, near1, near_s, near_r, where)

    up_other = (sp + 2, 2 * x)
    pl.when(has_up & (c == 1))(lambda: near(up_other).start())
    pl.when(has_up)(lambda: far(0, 0, 2, above).start())
    pl.when(c == 0)(lambda: near(side).start())
    pl.when(c == 0)(lambda: far(1, 0, 1, side).start())

    for d in range(1, 5):
        @pl.when(rank < d)
        def _(d=d):
            far2[d] = jnp.zeros(far2.shape[1:], far2.dtype)

    @pl.when(rank < 1)
    def _():
        near1[...] = jnp.zeros(near1.shape, near1.dtype)

    for d in range(2, nz):
        relay(2, d)
    @pl.when(has_down)
    def _():
        far(0, 0, 2, above).wait_recv()
        pl.when(has_up)(lambda: far(2, 2, 4, above).start())
        pl.when(c == 0)(lambda: far(3, 2, 3, side).start())
        pl.when(c == 1)(lambda: far(3, 2, 1, side).start())

    o_y().wait()
    o_x().start()
    others(2)

    def keep_query(index, rows, g, part):
        queries[g, rows, :] = part.astype(jnp.bfloat16)

    project(2, keep_query)

    scale = DH ** (-0.5)
    far_off = 1 << 24

    def dots(q, k):
        return lax.dot_general(q, k, (((1,), (1,)), ((), ())), preferred_element_type=jnp.float32)

    def iota(shape, axis):
        return lax.broadcasted_iota(jnp.int32, shape, axis)

    def soft(scores, time_q, time_k, reach, first):
        gap = time_q - jnp.where(time_k >= first, time_k, far_off)
        scores = jnp.where((gap >= 0) & (gap <= reach), scores * scale, -jnp.inf)
        top = jnp.max(scores, axis=-1, keepdims=True)
        weight = jnp.exp(scores - top)
        return top, jnp.sum(weight, axis=-1, keepdims=True), weight.astype(jnp.bfloat16)

    def near_groups(index, carry):
        begin = index * block
        rows = pl.ds(pl.multiple_of(begin, block), block)
        q = queries[0, rows, :]
        tails = pl.ds(tok_rows, tail)
        scores = jnp.concatenate([dots(q, near1[0, tails, :]), dots(q, pair0[0])], axis=1)
        lane = iota((1, tail + tok_rows), 1)
        time_k = jnp.where(lane < tail, tail_time(lane & (tail - 1)), row_time(lane - tail))
        time_q = row_time(iota((block, 1), 0) + begin)
        top0, sum0, weight = soft(scores, time_q, time_k, WIN1, -rank * tok_rows)
        got0 = jnp.dot(weight[:, :tail], near1[1, tails, :], preferred_element_type=jnp.float32)
        got0 += jnp.dot(weight[:, tail:], pair0[1], preferred_element_type=jnp.float32)
        q = queries[1, rows, :]
        scores = jnp.concatenate([dots(q, near1[0, rows, :]), dots(q, send1[0, rows, :])], axis=1)

        def step_of(place):
            return 4 * (place & (sub - 1)) + (place >> sub_log)

        lane = iota((1, 2 * block), 1)
        step_k = step_of(lane & (block - 1)) + jnp.where(lane < block, -block, 0)
        top1, sum1, weight = soft(
            scores, step_of(iota((block, 1), 0)), step_k, WIN2 // SECOND_DILATION, -rank * block
        )
        got1 = jnp.dot(weight[:, :block], near1[1, rows, :], preferred_element_type=jnp.float32)
        got1 += jnp.dot(weight[:, block:], send1[1, rows, :], preferred_element_type=jnp.float32)
        top = jnp.maximum(top0, top1)
        f0, f1 = jnp.exp(top0 - top), jnp.exp(top1 - top)
        got01[rows, :] = f0 * got0 + f1 * got1
        top01[rows, :] = top
        sum01[rows, :] = f0 * sum0 + f1 * sum1
        return carry

    def far_group(index, carry):
        begin = index * block
        rows = pl.ds(pl.multiple_of(begin, block), block)
        all_scores = []
        for b in range(4):
            here = pl.ds(pl.multiple_of(begin + b * sub, sub), sub)
            keys = jnp.concatenate([far2[d, 0, here, :] for d in (4, 3, 2, 1, 0)], axis=0)
            all_scores.append(dots(queries[2, here, :], keys))
        scores = jnp.concatenate(all_scores, axis=0)
        step_q = iota((block, 1), 0) & (sub - 1)
        step_k = iota((1, 5 * sub), 1) - 4 * sub
        top2, sum2, weight = soft(scores, step_q, step_k, WIN3 // THIRD_DILATION, -rank * sub)
        got = []
        for b in range(4):
            here = pl.ds(pl.multiple_of(begin + b * sub, sub), sub)
            vals = jnp.concatenate([far2[d, 1, here, :] for d in (4, 3, 2, 1, 0)], axis=0)
            got.append(jnp.dot(weight[b * sub : (b + 1) * sub], vals, preferred_element_type=jnp.float32))
        got2 = jnp.concatenate(got, axis=0)
        top1 = top01[rows, :]
        top = jnp.maximum(top1, top2)
        f1, f2 = jnp.exp(top1 - top), jnp.exp(top2 - top)
        total = f1 * sum01[rows, :] + f2 * sum2
        mine[0, rows, :] = ((f1 * got01[rows, :] + f2 * got2) / total).astype(jnp.bfloat16)
        return carry

    pl.when(rank >= 1)(lambda: near(side).wait_recv())
    lax.fori_loop(0, SECOND_DILATION, near_groups, 0)
    o_x().wait()
    o_c().start()

    @pl.when(z >= 2)
    def _():
        far(2, 2, 4, above).wait_recv()
        pl.when(c == 1)(lambda: far(4, 4, 3, side).start())

    pl.when(rank >= 1)(lambda: far(1, 0, 1, side).wait_recv())
    pl.when(rank >= 3)(lambda: far(4, 4, 3, side).wait_recv())
    lax.fori_loop(0, SECOND_DILATION, far_group, 0)

    t = iota((tok_rows, tok_rows), 0)
    p = row_time(iota((tok_rows, tok_rows), 1))
    mine[1] = jnp.dot(
        jnp.where(p == t, 1.0, 0.0).astype(jnp.bfloat16), mine[0], preferred_element_type=jnp.float32
    ).astype(jnp.bfloat16)
    head = 2 * x + y
    quarter = tok_rows // 4

    def deal(k):
        return send(mine.at[1, pl.ds(k * quarter, quarter), :], heads_in.at[head], head_s.at[k], head_r.at[head], (2 * z + c, k))

    def deal_self(k):
        return pltpu.make_async_copy(mine.at[1, pl.ds(k * quarter, quarter), :], heads_in.at[head], head_r.at[head])

    for k in range(4):
        self_here = (y == c) & (tp == k)
        pl.when(self_here)(lambda k=k: deal_self(k).start())
        pl.when(jnp.logical_not(self_here))(lambda k=k: deal(k).start())

    o_c().wait()
    for h in range(4):
        pltpu.make_async_copy(heads_in.at[h], heads_in.at[h], head_r.at[h]).wait()
    for zz in range(nz):
        for yy in range(2):
            acc = None
            for h in range(4):
                one = jnp.dot(heads_in[h], out_rows[h % 2, h // 2, yy, zz], preferred_element_type=jnp.float32)
                acc = one if acc is None else acc + one
            width = w_out.shape[1]
            s = 2 * zz + yy
            out[:, s * width : (s + 1) * width] = acc.astype(jnp.bfloat16)

    for k in range(4):
        self_here = (y == c) & (tp == k)
        pl.when(jnp.logical_not(self_here))(lambda k=k: deal(k).wait_send())

    @pl.when(jnp.logical_not(stays))
    def _():
        for a in range(3):
            swapped(a).wait_send()
        tok_swapped().wait_send()

    for a in range(4):
        for zz in range(nz):
            pl.when(has_up & (zz <= z))(lambda a=a, zz=zz: go(a, zz, "up").wait_send())
            pl.when(has_down & (zz >= z))(lambda a=a, zz=zz: go(a, zz, "down").wait_send())
            if a < 3:
                go(a, zz, "side").wait_send()
    pl.when(has_up)(lambda: far(0, 0, 2, above).wait_send())
    pl.when(c == 0)(lambda: far(1, 0, 1, side).wait_send())
    pl.when((c == 0) | has_up)(lambda: near(side).wait_send())
    pl.when(has_down & has_up)(lambda: far(2, 2, 4, above).wait_send())
    pl.when(has_down)(lambda: far(3, 2, 3, side).wait_send())
    pl.when((z >= 2) & (c == 1))(lambda: far(4, 4, 3, side).wait_send())


def fits_kernel(n_sp, n_tp, tokens, w_query, w_out):
    tok_rows, depth = tokens.shape
    return (
        n_sp % 2 == 0
        and n_tp == 4
        and w_query.shape[1] == GROUPS * DH
        and w_out.shape[0] == DH
        and w_out.shape[1] % 128 == 0
        and w_query.shape[0] % 16 == 0
        and tok_rows == WIN2
        and 4 * tok_rows == WIN3
        and 4 * WIN1 == tok_rows
    )


def one_kernel(n_sp, tokens, w_query, w_key, w_value, w_out):
    nz = n_sp // 2
    tok_rows, depth = tokens.shape
    cols = w_query.shape[1]
    bf, dma = jnp.bfloat16, pltpu.SemaphoreType.DMA
    return pl.pallas_call(
        functools.partial(layer_kernel, nz),
        out_shape=jax.ShapeDtypeStruct((tok_rows // 4, w_out.shape[1] * n_sp), bf),
        in_specs=[pl.BlockSpec(memory_space=pltpu.HBM)] * 5,
        out_specs=pl.BlockSpec(memory_space=pltpu.VMEM),
        scratch_shapes=[
            pltpu.VMEM((3, depth, cols), bf),
            pltpu.VMEM((tok_rows, depth), bf),
            pltpu.VMEM((tok_rows, depth), bf),
            pltpu.VMEM((tok_rows, DH), jnp.float32),
            pltpu.VMEM((tok_rows, DH), jnp.float32),
            pltpu.VMEM((GROUPS, tok_rows, DH), bf),
            pltpu.VMEM((2, tok_rows, DH), bf),
            pltpu.VMEM((2, tok_rows + WIN1, DH), bf),
            pltpu.VMEM((2, tok_rows + WIN1, DH), bf),
            pltpu.VMEM((5, 2, tok_rows, DH), bf),
            pltpu.VMEM((2, 2, 2, nz, *w_out.shape), bf),
            pltpu.VMEM((2, tok_rows, DH), bf),
            pltpu.VMEM((4, tok_rows // 4, DH), bf),
            pltpu.VMEM((tok_rows, DH), jnp.float32),
            pltpu.VMEM((tok_rows, 1), jnp.float32),
            pltpu.VMEM((tok_rows, 1), jnp.float32),
            dma((4,)), dma, dma((3, n_sp)),
            dma((4, nz)), dma((4, nz)), dma((3, nz)),
            dma((nz,)), dma((3,)), dma((3,)),
            dma((5,)), dma((5,)), dma, dma,
            dma((4,)), dma((4,)),
        ],
        compiler_params=pltpu.CompilerParams(
            collective_id=0, has_side_effects=True, vmem_limit_bytes=60 * 1024 * 1024
        ),
    )(tokens, w_key, w_value, w_query, w_out)


def on_mesh(n_sp, n_tp, *operands):
    tokens, w_query, _, _, w_out = operands
    if fits_kernel(n_sp, n_tp, tokens, w_query, w_out):
        return one_kernel(n_sp, *operands)
    return on_device(*operands)


def solution(mesh):
    placed = (P("sp", None), P("sp", "tp"), P("sp", "tp"), P("sp", "tp"), P("tp", "sp"))
    body = functools.partial(on_mesh, mesh.shape["sp"], mesh.shape["tp"])
    return jax.shard_map(
        body, mesh=mesh, in_specs=placed, out_specs=P(("sp", "tp"), None), check_vma=False
    )
```

```python
import functools
import math

import jax
import jax.numpy as jnp
from jax import lax
from jax.experimental import pallas as pl
from jax.experimental.pallas import tpu as pltpu
from jax.sharding import PartitionSpec as P

GROUPS = 3
DH = 128
WIN1 = 128
WIN2 = 512
WIN3 = 2048
SECOND_DILATION = 4
THIRD_DILATION = 16


ROPE_BASE = 500000.0


def from_behind(block, axis, distance):
    devices = range(lax.axis_size(axis))
    route = [(i - distance, i) for i in devices if i - distance in devices]
    return lax.ppermute(block, axis, route)


def rotate(projected, offset):
    tok_rows = projected.shape[0]
    head_size = projected.shape[-1]
    half_size = head_size // 2
    positions = (offset + jnp.arange(tok_rows, dtype=jnp.int32)).astype(jnp.float32)
    frequency = 1.0 / ROPE_BASE ** (jnp.arange(0, head_size, 2, dtype=jnp.float32) / head_size)
    angles = (positions[:, None] * frequency[None, :]).reshape(tok_rows, 1, 1, half_size)
    cosine = jnp.cos(angles)
    sine_part = jnp.sin(angles)
    first_half = projected[..., :half_size]
    second_half = projected[..., half_size:]
    return jnp.concatenate(
        [
            first_half * cosine - second_half * sine_part,
            second_half * cosine + first_half * sine_part,
        ],
        axis=-1,
    )


def window_attend(query_part, buffer, steps, stride, offset):
    tok_rows, heads_here, head_size = query_part.shape
    sub_rows = tok_rows // stride
    key_rows = buffer.shape[1] // stride
    query_sub = query_part.reshape(sub_rows, stride, heads_here, head_size).transpose(1, 2, 0, 3)
    pair_sub = buffer.reshape(2, key_rows, stride, heads_here, head_size).transpose(0, 2, 3, 1, 4)
    block_rows = math.gcd(sub_rows, steps) if sub_rows > steps else sub_rows
    block_list = sub_rows // block_rows
    query_blocks = query_sub.reshape(stride, heads_here, block_list, block_rows, head_size)
    key_blocks = jnp.stack(
        [
            pair_sub[:, :, :, index * block_rows : index * block_rows + block_rows + steps]
            for index in range(block_list)
        ],
        axis=3,
    )
    scores = jnp.einsum(
        "zhnqe,zhnke->zhnqk", query_blocks, key_blocks[0], preferred_element_type=jnp.float32
    ) * head_size ** (-0.5)
    query_index = (jnp.arange(block_list, dtype=jnp.int32) * block_rows)[
        :, None, None
    ] + jnp.arange(block_rows, dtype=jnp.int32)[None, :, None]
    key_index = (jnp.arange(block_list, dtype=jnp.int32) * block_rows)[:, None, None] + jnp.arange(
        block_rows + steps, dtype=jnp.int32
    )[None, None, :]
    spacing = query_index + steps - key_index
    residue = jnp.arange(stride, dtype=jnp.int32)[:, None, None, None]
    key_position = offset + (key_index[None] - steps) * stride + residue
    allowed = (spacing[None] >= 0) & (spacing[None] <= steps) & (key_position >= 0)
    scores = jnp.where(allowed[:, None], scores, -jnp.inf)
    row_max = jnp.max(scores, axis=-1)
    exponent = jnp.exp(scores - row_max[..., None])
    totals = jnp.sum(exponent, axis=-1)
    probs = (exponent / totals[..., None]).astype(jnp.bfloat16)
    mixed = jnp.einsum(
        "zhnqk,zhnke->zhnqe", probs, key_blocks[1], preferred_element_type=jnp.float32
    )
    mixed = mixed.reshape(stride, heads_here, sub_rows, head_size).transpose(2, 0, 1, 3)
    log_total = (row_max + jnp.log(totals)).reshape(stride, heads_here, sub_rows).transpose(2, 0, 1)
    return (mixed.reshape(tok_rows, heads_here, head_size), log_total.reshape(tok_rows, heads_here))


def reach_back(key_value, distance_max):
    tok_rows = key_value.shape[1]
    gathered = key_value
    pieces_held = 1
    while pieces_held < distance_max + 1:
        slice_share = min(pieces_held, distance_max + 1 - pieces_held)
        arrived = from_behind(
            gathered[:, gathered.shape[1] - slice_share * tok_rows :], "sp", pieces_held
        )
        gathered = jnp.concatenate([arrived, gathered], axis=1)
        pieces_held = pieces_held + slice_share
    return gathered


def on_device(tokens, w_query, w_key, w_value, w_out):
    tok_rows = tokens.shape[0]
    heads_here = w_out.shape[0] // DH
    offset = lax.axis_index("sp") * tok_rows
    weight_parts = (
        lax.all_gather(w_query, "sp", axis=0, tiled=True),
        lax.all_gather(w_key, "sp", axis=0, tiled=True),
        lax.all_gather(w_value, "sp", axis=0, tiled=True),
    )
    query_raw, key_raw, value_raw = tuple(
        (
            jnp.dot(tokens, weight_rows, preferred_element_type=jnp.float32)
            for weight_rows in weight_parts
        )
    )
    head_shape = (tok_rows, heads_here, GROUPS, DH)
    queries = rotate(query_raw.reshape(head_shape), offset).astype(jnp.bfloat16)
    keys_all = rotate(key_raw.reshape(head_shape), offset).astype(jnp.bfloat16)
    values_all = value_raw.astype(jnp.bfloat16).reshape(head_shape)
    windows = (WIN1, WIN2, WIN3)
    step_sizes = (1, SECOND_DILATION, THIRD_DILATION)
    outputs = []
    log_totals = []
    for group_index in range(GROUPS):
        key_value = jnp.stack([keys_all[:, :, group_index], values_all[:, :, group_index]])
        key_value = key_value.reshape(2, tok_rows, heads_here * DH)
        window = windows[group_index]
        if group_index == 0:
            near_rows = from_behind(key_value[:, tok_rows - window :], "sp", 1)
            buffer = jnp.concatenate([near_rows, key_value], axis=1)
        else:
            distance_max = (window + tok_rows - 1) // tok_rows
            buffer = reach_back(key_value, distance_max)
        group_out, log_total = window_attend(
            queries[:, :, group_index],
            buffer,
            window // step_sizes[group_index],
            step_sizes[group_index],
            offset,
        )
        outputs.append(group_out)
        log_totals.append(log_total)
    group_weights = jax.nn.softmax(jnp.stack(log_totals), axis=0)
    merged = jnp.sum(group_weights[..., None] * jnp.stack(outputs), axis=0).astype(jnp.bfloat16)
    merged = merged.reshape(tok_rows, heads_here * DH)
    w_whole = lax.all_gather(w_out, "sp", axis=1, tiled=True)
    return lax.psum_scatter(
        jnp.dot(merged, w_whole, preferred_element_type=jnp.float32).astype(jnp.bfloat16),
        "tp",
        scatter_dimension=0,
        tiled=True,
    )


def layer_kernel(
    nz,
    tokens, w_key, w_value, w_query, w_out, out,
    weights, tok_in, tok_turned, cosine, sine, queries, pair0, send1, near1, far2,
    out_rows, mine, heads_in, got01, top01, sum01,
    swap_s, tok_r, w_r, up_s, down_s, side_s, o_r, o_s, o_r2, far_s, far_r, near_s, near_r, head_s, head_r,
):
    tok_rows, depth = tokens.shape
    k_rows, cols = w_key.shape
    sub = tok_rows // THIRD_DILATION
    sub_log = sub.bit_length() - 1
    block = tok_rows // SECOND_DILATION
    tail = WIN1
    sp, tp = lax.axis_index("sp"), lax.axis_index("tp")
    z, y = sp // 2, sp % 2
    x, c = tp // 2, tp % 2
    rank = 2 * z + c
    side = (sp, 2 * x + 1 - c)
    above = (sp + 2, tp)
    below = (sp - 2, tp)
    partner = (2 * z + 1 - y, 2 * x + 1 - c)
    stays = c == y
    has_up, has_down = z < nz - 1, z > 0

    def send(src, dst, s_sem, r_sem, where):
        return pltpu.make_async_remote_copy(
            src_ref=src, dst_ref=dst, send_sem=s_sem, recv_sem=r_sem,
            device_id=where, device_id_type=pl.DeviceIdType.MESH,
        )

    parts = (w_key, w_value, w_query)

    def chunk(a, s):
        return weights.at[a, pl.ds(pl.multiple_of(s * k_rows, k_rows), k_rows), :]

    def o_chunk(zz):
        return out_rows.at[c, x, y, zz]

    def swapped(a):
        there = 2 * z + 1 - c
        return send(parts[a], chunk(a, there), swap_s.at[a], w_r.at[a, there], partner)

    def tok_swapped():
        return send(tokens, tok_in, swap_s.at[3], tok_r, partner)

    def kept(a):
        return pltpu.make_async_copy(parts[a], chunk(a, rank), w_r.at[a, rank])

    def o_kept():
        return pltpu.make_async_copy(w_out, o_chunk(z), o_r.at[z])

    def tok_kept():
        return pltpu.make_async_copy(tokens, tok_in, tok_r)

    @pl.when(stays)
    def _():
        for a in range(3):
            kept(a).start()
        tok_kept().start()

    o_kept().start()

    barrier = pltpu.get_barrier_semaphore()

    def greet(where):
        pl.semaphore_signal(barrier, inc=1, device_id=where, device_id_type=pl.DeviceIdType.MESH)

    for dy in range(2):
        for dx in range(2):
            for dc in range(2):
                if dy + dx + dc:
                    greet((2 * z + (y + dy) % 2, 2 * ((x + dx) % 2) + (c + dc) % 2))
    pl.when(has_up)(lambda: greet(above))
    pl.when(has_down)(lambda: greet(below))
    pl.when(has_up & (c == 1))(lambda: greet((sp + 2, 2 * x)))
    pl.when(has_down & (c == 0))(lambda: greet((sp - 2, 2 * x + 1)))
    greeters = 7 + jnp.where(has_up, 1 + c, 0) + jnp.where(has_down, 2 - c, 0)
    pl.semaphore_wait(barrier, greeters)

    @pl.when(jnp.logical_not(stays))
    def _():
        swapped(0).start()
        swapped(1).start()
        tok_swapped().start()
        swapped(2).start()

    def go(a, zz, kind):
        s = 2 * zz + c
        ref = chunk(a, s) if a < 3 else o_chunk(zz)
        r_sem = w_r.at[a, s] if a < 3 else o_r.at[zz]
        s_sem = {"up": up_s, "down": down_s, "side": side_s}[kind].at[a, zz]
        return send(ref, ref, s_sem, r_sem, {"up": above, "down": below, "side": side}[kind])

    def own(a):
        if a < 3:
            pl.when(stays)(lambda: kept(a).wait())
            pl.when(jnp.logical_not(stays))(lambda: go(a, z, "side").wait_recv())
        else:
            o_kept().wait()
        pl.when(has_up)(lambda: go(a, z, "up").start())
        pl.when(has_down)(lambda: go(a, z, "down").start())
        if a < 3:
            go(a, z, "side").start()

    def relay(a, d):
        @pl.when(z - d >= 0)
        def _():
            go(a, z - d, "up").wait_recv()
            pl.when(has_up)(lambda: go(a, z - d, "up").start())
            if a < 3:
                go(a, z - d, "side").start()

        @pl.when(z + d < nz)
        def _():
            go(a, z + d, "down").wait_recv()
            pl.when(has_down)(lambda: go(a, z + d, "down").start())
            if a < 3:
                go(a, z + d, "side").start()

    def others(a):
        for zz in range(nz):
            s = 2 * zz + 1 - c
            send(chunk(a, s), chunk(a, s), side_s.at[a, zz], w_r.at[a, s], side).wait_recv()

    def row_time(p):
        b, i = p >> sub_log, p & (sub - 1)
        return THIRD_DILATION * i + (b >> 2) + SECOND_DILATION * (b & 3)

    def tail_time(u):
        per = tail // THIRD_DILATION
        b, i = u >> (per.bit_length() - 1), u & (per - 1)
        return THIRD_DILATION * (sub - per + i) + (b >> 2) + SECOND_DILATION * (b & 3) - tok_rows

    own(0)
    own(1)

    pair_at = lax.broadcasted_iota(jnp.int32, (1, DH), 1) & (DH // 2 - 1)
    freq = jnp.exp(pair_at.astype(jnp.float32) * (-2.0 * math.log(ROPE_BASE) / DH))

    def angles(index, carry):
        rows = pl.ds(pl.multiple_of(index * block, block), block)
        p = lax.broadcasted_iota(jnp.int32, (block, DH), 0) + index * block
        angle = (row_time(p) + rank * tok_rows).astype(jnp.float32) * freq
        lane = lax.broadcasted_iota(jnp.int32, (block, DH), 1)
        cosine[rows, :] = jnp.cos(angle)
        turned = jnp.sin(angle)
        sine[rows, :] = jnp.where(lane < DH // 2, -turned, turned)
        return carry

    lax.fori_loop(0, SECOND_DILATION, angles, 0)

    def relay_all(a, following):
        for d in range(1, nz):
            if d == nz - 1 and following is not None:
                own(following)
            relay(a, d)

    def order(source):
        p = row_time(lax.broadcasted_iota(jnp.int32, (tok_rows, tok_rows), 0))
        t = lax.broadcasted_iota(jnp.int32, (tok_rows, tok_rows), 1)
        pick = jnp.where(p == t, 1.0, 0.0).astype(jnp.bfloat16)

        def piece(index, carry):
            at = pl.ds(pl.multiple_of(index * 256, 256), 256)
            tok_turned[:, at] = jnp.dot(
                pick, source[:, at], preferred_element_type=jnp.float32
            ).astype(jnp.bfloat16)
            return carry

        lax.fori_loop(0, depth // 256, piece, 0)

    @pl.when(stays)
    def _():
        tok_kept().wait()
        order(tok_in)

    def o_y():
        return send(out_rows.at[c, x, y], out_rows.at[c, x, y], o_s.at[0], o_r2.at[0], (2 * z + 1 - y, tp))

    def o_x():
        return send(out_rows.at[c, x], out_rows.at[c, x], o_s.at[1], o_r2.at[1], (sp, 2 * (1 - x) + c))

    def o_c():
        return send(out_rows.at[c], out_rows.at[c], o_s.at[2], o_r2.at[2], side)

    relay_all(0, 3)
    relay_all(3, None)
    o_y().start()
    relay_all(1, 2)
    relay(2, 1)

    @pl.when(jnp.logical_not(stays))
    def _():
        tok_swapped().wait_recv()
        order(tok_in)

    def project(a, store):
        def piece(index, carry):
            rows = pl.ds(pl.multiple_of(index * block, block), block)
            raw = jnp.dot(tok_turned[rows, :], weights[a], preferred_element_type=jnp.float32)
            for g in range(GROUPS):
                part = raw[:, g * DH : (g + 1) * DH]
                if a != 1:
                    part = part * cosine[rows, :] + pltpu.roll(part, DH // 2, 1) * sine[rows, :]
                store(index, rows, g, part)
            return carry

        lax.fori_loop(0, SECOND_DILATION, piece, 0)

    def keep_pair(which):
        def store(index, rows, g, part):
            if g == 2:
                far2[0, which, rows, :] = part.astype(jnp.bfloat16)
            elif g == 1:
                send1[which, rows, :] = part.astype(jnp.bfloat16)
            else:
                pair0[which, rows, :] = part.astype(jnp.bfloat16)
                per = tail // THIRD_DILATION
                last = jnp.concatenate(
                    [part[b * sub + sub - per : (b + 1) * sub] for b in range(4)], axis=0
                )
                at = pl.ds(pl.multiple_of(tok_rows + index * 4 * per, 4 * per), 4 * per)
                send1[which, at, :] = last.astype(jnp.bfloat16)

        return store

    others(0)
    project(0, keep_pair(0))
    if nz > 2:
        relay(2, 2)
    others(1)
    project(1, keep_pair(1))

    def far(index, src, dst, where):
        return send(far2.at[src], far2.at[dst], far_s.at[index], far_r.at[dst], where)

    def near(where):
        return send(send1, near1, near_s, near_r, where)

    up_other = (sp + 2, 2 * x)
    pl.when(has_up & (c == 1))(lambda: near(up_other).start())
    pl.when(has_up)(lambda: far(0, 0, 2, above).start())
    pl.when(c == 0)(lambda: near(side).start())
    pl.when(c == 0)(lambda: far(1, 0, 1, side).start())

    for d in range(1, 5):
        @pl.when(rank < d)
        def _(d=d):
            far2[d] = jnp.zeros(far2.shape[1:], far2.dtype)

    @pl.when(rank < 1)
    def _():
        near1[...] = jnp.zeros(near1.shape, near1.dtype)

    for d in range(3, nz):
        relay(2, d)
    @pl.when(has_down)
    def _():
        far(0, 0, 2, above).wait_recv()
        pl.when(has_up)(lambda: far(2, 2, 4, above).start())
        pl.when(c == 0)(lambda: far(3, 2, 3, side).start())
        pl.when(c == 1)(lambda: far(3, 2, 1, side).start())

    o_y().wait()
    o_x().start()
    others(2)

    def keep_query(index, rows, g, part):
        queries[g, rows, :] = part.astype(jnp.bfloat16)

    project(2, keep_query)

    scale = DH ** (-0.5)
    far_off = 1 << 24

    def dots(q, k):
        return lax.dot_general(q, k, (((1,), (1,)), ((), ())), preferred_element_type=jnp.float32)

    def iota(shape, axis):
        return lax.broadcasted_iota(jnp.int32, shape, axis)

    def soft(scores, time_q, time_k, reach, first):
        gap = time_q - jnp.where(time_k >= first, time_k, far_off)
        scores = jnp.where((gap >= 0) & (gap <= reach), scores * scale, -jnp.inf)
        top = jnp.max(scores, axis=-1, keepdims=True)
        weight = jnp.exp(scores - top)
        return top, jnp.sum(weight, axis=-1, keepdims=True), weight.astype(jnp.bfloat16)

    def near_groups(index, carry):
        begin = index * block
        rows = pl.ds(pl.multiple_of(begin, block), block)
        q = queries[0, rows, :]
        tails = pl.ds(tok_rows, tail)
        scores = jnp.concatenate([dots(q, near1[0, tails, :]), dots(q, pair0[0])], axis=1)
        lane = iota((1, tail + tok_rows), 1)
        time_k = jnp.where(lane < tail, tail_time(lane & (tail - 1)), row_time(lane - tail))
        time_q = row_time(iota((block, 1), 0) + begin)
        top0, sum0, weight = soft(scores, time_q, time_k, WIN1, -rank * tok_rows)
        got0 = jnp.dot(weight[:, :tail], near1[1, tails, :], preferred_element_type=jnp.float32)
        got0 += jnp.dot(weight[:, tail:], pair0[1], preferred_element_type=jnp.float32)
        q = queries[1, rows, :]
        scores = jnp.concatenate([dots(q, near1[0, rows, :]), dots(q, send1[0, rows, :])], axis=1)

        def step_of(place):
            return 4 * (place & (sub - 1)) + (place >> sub_log)

        lane = iota((1, 2 * block), 1)
        step_k = step_of(lane & (block - 1)) + jnp.where(lane < block, -block, 0)
        top1, sum1, weight = soft(
            scores, step_of(iota((block, 1), 0)), step_k, WIN2 // SECOND_DILATION, -rank * block
        )
        got1 = jnp.dot(weight[:, :block], near1[1, rows, :], preferred_element_type=jnp.float32)
        got1 += jnp.dot(weight[:, block:], send1[1, rows, :], preferred_element_type=jnp.float32)
        top = jnp.maximum(top0, top1)
        f0, f1 = jnp.exp(top0 - top), jnp.exp(top1 - top)
        got01[rows, :] = f0 * got0 + f1 * got1
        top01[rows, :] = top
        sum01[rows, :] = f0 * sum0 + f1 * sum1
        return carry

    def far_group(slots, last, index, carry):
        begin = index * block
        rows = pl.ds(pl.multiple_of(begin, block), block)
        heres = [pl.ds(pl.multiple_of(begin + b * sub, sub), sub) for b in range(4)]
        all_scores = []
        for here in heres:
            keys = jnp.concatenate([far2[d, 0, here, :] for d in slots], axis=0)
            all_scores.append(dots(queries[2, here, :], keys))
        scores = jnp.concatenate(all_scores, axis=0)
        time_q = iota((block, 1), 0) & (sub - 1)
        time_k = iota((1, len(slots) * sub), 1) - slots[0] * sub
        gap = time_q - jnp.where(time_k >= -rank * sub, time_k, far_off)
        allowed = (gap >= 0) & (gap <= WIN3 // THIRD_DILATION)
        scores = jnp.where(allowed, scores * scale, -jnp.inf)
        before = top01[rows, :]
        top = jnp.maximum(before, jnp.max(scores, axis=-1, keepdims=True))
        factor = jnp.exp(before - top)
        weight = jnp.exp(scores - top)
        total = factor * sum01[rows, :] + jnp.sum(weight, axis=-1, keepdims=True)
        weight = weight.astype(jnp.bfloat16)
        got = []
        for b, here in enumerate(heres):
            vals = jnp.concatenate([far2[d, 1, here, :] for d in slots], axis=0)
            got.append(jnp.dot(weight[b * sub : (b + 1) * sub], vals, preferred_element_type=jnp.float32))
        both = factor * got01[rows, :] + jnp.concatenate(got, axis=0)
        if last:
            mine[0, rows, :] = (both / total).astype(jnp.bfloat16)
        else:
            got01[rows, :] = both
            top01[rows, :] = top
            sum01[rows, :] = total
        return carry

    pl.when(rank >= 1)(lambda: near(side).wait_recv())
    lax.fori_loop(0, SECOND_DILATION, near_groups, 0)
    o_x().wait()
    o_c().start()

    pl.when(rank >= 1)(lambda: far(1, 0, 1, side).wait_recv())
    lax.fori_loop(0, SECOND_DILATION, functools.partial(far_group, (2, 1, 0), False), 0)

    @pl.when(z >= 2)
    def _():
        far(2, 2, 4, above).wait_recv()
        pl.when(c == 1)(lambda: far(4, 4, 3, side).start())

    pl.when(rank >= 3)(lambda: far(4, 4, 3, side).wait_recv())
    lax.fori_loop(0, SECOND_DILATION, functools.partial(far_group, (4, 3), True), 0)

    t = iota((tok_rows, tok_rows), 0)
    p = row_time(iota((tok_rows, tok_rows), 1))
    mine[1] = jnp.dot(
        jnp.where(p == t, 1.0, 0.0).astype(jnp.bfloat16), mine[0], preferred_element_type=jnp.float32
    ).astype(jnp.bfloat16)
    head = 2 * x + y
    quarter = tok_rows // 4

    def deal(k):
        return send(mine.at[1, pl.ds(k * quarter, quarter), :], heads_in.at[head], head_s.at[k], head_r.at[head], (2 * z + c, k))

    def deal_self(k):
        return pltpu.make_async_copy(mine.at[1, pl.ds(k * quarter, quarter), :], heads_in.at[head], head_r.at[head])

    for k in range(4):
        self_here = (y == c) & (tp == k)
        pl.when(self_here)(lambda k=k: deal_self(k).start())
        pl.when(jnp.logical_not(self_here))(lambda k=k: deal(k).start())

    o_c().wait()
    for h in range(4):
        pltpu.make_async_copy(heads_in.at[h], heads_in.at[h], head_r.at[h]).wait()
    for zz in range(nz):
        for yy in range(2):
            acc = None
            for h in range(4):
                one = jnp.dot(heads_in[h], out_rows[h % 2, h // 2, yy, zz], preferred_element_type=jnp.float32)
                acc = one if acc is None else acc + one
            width = w_out.shape[1]
            s = 2 * zz + yy
            out[:, s * width : (s + 1) * width] = acc.astype(jnp.bfloat16)

    for k in range(4):
        self_here = (y == c) & (tp == k)
        pl.when(jnp.logical_not(self_here))(lambda k=k: deal(k).wait_send())

    @pl.when(jnp.logical_not(stays))
    def _():
        for a in range(3):
            swapped(a).wait_send()
        tok_swapped().wait_send()

    for a in range(4):
        for zz in range(nz):
            pl.when(has_up & (zz <= z))(lambda a=a, zz=zz: go(a, zz, "up").wait_send())
            pl.when(has_down & (zz >= z))(lambda a=a, zz=zz: go(a, zz, "down").wait_send())
            if a < 3:
                go(a, zz, "side").wait_send()
    pl.when(has_up)(lambda: far(0, 0, 2, above).wait_send())
    pl.when(c == 0)(lambda: far(1, 0, 1, side).wait_send())
    pl.when((c == 0) | has_up)(lambda: near(side).wait_send())
    pl.when(has_down & has_up)(lambda: far(2, 2, 4, above).wait_send())
    pl.when(has_down)(lambda: far(3, 2, 3, side).wait_send())
    pl.when((z >= 2) & (c == 1))(lambda: far(4, 4, 3, side).wait_send())


def fits_kernel(n_sp, n_tp, tokens, w_query, w_out):
    tok_rows, depth = tokens.shape
    return (
        n_sp % 2 == 0
        and n_tp == 4
        and w_query.shape[1] == GROUPS * DH
        and w_out.shape[0] == DH
        and w_out.shape[1] % 128 == 0
        and w_query.shape[0] % 16 == 0
        and tok_rows == WIN2
        and 4 * tok_rows == WIN3
        and 4 * WIN1 == tok_rows
    )


def one_kernel(n_sp, tokens, w_query, w_key, w_value, w_out):
    nz = n_sp // 2
    tok_rows, depth = tokens.shape
    cols = w_query.shape[1]
    bf, dma = jnp.bfloat16, pltpu.SemaphoreType.DMA
    return pl.pallas_call(
        functools.partial(layer_kernel, nz),
        out_shape=jax.ShapeDtypeStruct((tok_rows // 4, w_out.shape[1] * n_sp), bf),
        in_specs=[pl.BlockSpec(memory_space=pltpu.HBM)] * 5,
        out_specs=pl.BlockSpec(memory_space=pltpu.VMEM),
        scratch_shapes=[
            pltpu.VMEM((3, depth, cols), bf),
            pltpu.VMEM((tok_rows, depth), bf),
            pltpu.VMEM((tok_rows, depth), bf),
            pltpu.VMEM((tok_rows, DH), jnp.float32),
            pltpu.VMEM((tok_rows, DH), jnp.float32),
            pltpu.VMEM((GROUPS, tok_rows, DH), bf),
            pltpu.VMEM((2, tok_rows, DH), bf),
            pltpu.VMEM((2, tok_rows + WIN1, DH), bf),
            pltpu.VMEM((2, tok_rows + WIN1, DH), bf),
            pltpu.VMEM((5, 2, tok_rows, DH), bf),
            pltpu.VMEM((2, 2, 2, nz, *w_out.shape), bf),
            pltpu.VMEM((2, tok_rows, DH), bf),
            pltpu.VMEM((4, tok_rows // 4, DH), bf),
            pltpu.VMEM((tok_rows, DH), jnp.float32),
            pltpu.VMEM((tok_rows, 1), jnp.float32),
            pltpu.VMEM((tok_rows, 1), jnp.float32),
            dma((4,)), dma, dma((3, n_sp)),
            dma((4, nz)), dma((4, nz)), dma((3, nz)),
            dma((nz,)), dma((3,)), dma((3,)),
            dma((5,)), dma((5,)), dma, dma,
            dma((4,)), dma((4,)),
        ],
        compiler_params=pltpu.CompilerParams(
            collective_id=0, has_side_effects=True, vmem_limit_bytes=60 * 1024 * 1024
        ),
    )(tokens, w_key, w_value, w_query, w_out)


def on_mesh(n_sp, n_tp, *operands):
    tokens, w_query, _, _, w_out = operands
    if fits_kernel(n_sp, n_tp, tokens, w_query, w_out):
        return one_kernel(n_sp, *operands)
    return on_device(*operands)


def solution(mesh):
    placed = (P("sp", None), P("sp", "tp"), P("sp", "tp"), P("sp", "tp"), P("tp", "sp"))
    body = functools.partial(on_mesh, mesh.shape["sp"], mesh.shape["tp"])
    return jax.shard_map(
        body, mesh=mesh, in_specs=placed, out_specs=P(("sp", "tp"), None), check_vma=False
    )
```
